32 devices in a mesh: ep: 32 (over z, y, x, core).
Axes of the slice: x: 2, y: 2, z: 4, core: 2. Of those that a mesh axis runs over, the one named last changes fastest.
Arguments:
- tokens: bfloat16 [768, 2048], P('ep'), may hold values from -6 to 6
- state: float32 [768, 16, 64, 64], P('ep'), may hold values from -4 to 4
- norm_gain: float32 [2048], replicated, may hold values from 0.1 to 1.9
- w_recept: bfloat16 [2048, 1024], replicated, may hold values from -0.125 to 0.125
- w_keys: bfloat16 [2048, 1024], replicated, may hold values from -0.125 to 0.125
- w_values: bfloat16 [2048, 1024], replicated, may hold values from -0.125 to 0.125
- decay_base: float32 [1024], replicated, may hold values from -3 to 3
- decay_first_matrix: bfloat16 [2048, 128], replicated, may hold values from -0.125 to 0.125
- decay_second_matrix: bfloat16 [128, 1024], replicated, may hold values from -0.5 to 0.5
- rate_base: float32 [1024], replicated, may hold values from -3 to 3
- rate_first_matrix: bfloat16 [2048, 128], replicated, may hold values from -0.125 to 0.125
- rate_second_matrix: bfloat16 [128, 1024], replicated, may hold values from -0.5 to 0.5
- head_gain: float32 [1024], replicated, may hold values from 0.1 to 1.9
- w_output: bfloat16 [1024, 2048], replicated, may hold values from -0.1875 to 0.1875
- second_gain: float32 [2048], replicated, may hold values from 0.1 to 1.9
- route_ids: int32 [768, 2], replicated, may hold values from 0 to 15, all different within a row; in each aligned block of 24 rows (0 to 23, 24 to 47, ...) at most 6 rows name the same one
- route_weights: float32 [768, 2], replicated, may hold values from 0.2 to 1
- expert_gate: bfloat16 [2048, 49152], P(None, 'ep'), may hold values from -0.125 to 0.125
- expert_up: bfloat16 [2048, 49152], P(None, 'ep'), may hold values from -0.125 to 0.125
- expert_down: bfloat16 [49152, 2048], P('ep'), may hold values from -0.109375 to 0.109375
Outputs:
- layer_out: bfloat16 [768, 2048], P('ep')
- new_state: float32 [768, 16, 64, 64], P('ep')
The draws below stay inside these ranges and needn't reach their ends.
Inputs may be any that keep to these rules, and one draw needn't show every extreme that they name: `route_ids`: each row names 2 different experts. Among the 24 rows of one device (aligned blocks), no expert is named by more than 6 rows, and in every draw some block names some expert exactly 6 times.
All inputs are finite; a program needn't handle non-finite values.
Results may differ from the reference program's by a relative error of at most 0.015.
Values may be sent and summed in bfloat16 or wider, within the bound.
A program may use at most 192 MiB of HBM per device.

```python
import math
import jax
import jax.numpy as jnp
import numpy as np
from jax import lax

MODEL_WIDTH = 2048
MIXER_HEADS = 16
HEAD_SIZE = 64
LOWRANK_WIDTH = 128
EXPERTS = 16
FF_E = 3072
TOPK = 2
SEQ_DEV = 24
CAP_DEV = 6
BATCH = 768
N_EP = 32


def levels(stream_key, dims, cuts, least, high):
    def one(axis_at, shards_of):
        heights = jax.random.uniform(jax.random.fold_in(jax.random.fold_in(stream_key, 6), axis_at), (shards_of,), jnp.float32, least / len(cuts), high / len(cuts))
        return jnp.repeat(jnp.exp(heights), dims[axis_at] // shards_of).reshape((-1,) + (1,) * (len(dims) - axis_at - 1))

    level = one(*cuts[0])
    for cut in cuts[1:]:
        level = level * one(*cut)
    return level


def assign_block(key, own, number, rows, amount, top, most, slope):
    order = jax.random.permutation(key, amount)
    heavy_load, usual = portions_of(amount, rows * top, most, slope, True), portions_of(amount, rows * top, most, slope, False)
    places = jnp.arange(amount)

    def named(lengths, turn):
        used = int((lengths > 0).sum())
        fixed = max(1, used // 4)
        moved = fixed + (places - fixed + turn * (used - fixed)) % max(1, amount - fixed)
        return jnp.zeros((amount,), jnp.int32).at[order[jnp.where(places < fixed, places, moved)]].set(jnp.asarray(lengths, jnp.int32))

    lengths = jnp.where(number % 4 == 0, named(heavy_load, number // 4), named(usual, number - number // 4 - 1))
    mixed = jax.random.permutation(jax.random.fold_in(own, 3), amount)
    donor, taker = mixed[0:amount // 2 * 2:2], mixed[1:amount // 2 * 2:2]
    room = jnp.minimum(lengths[donor] - 1, most - lengths[taker]) // 2
    room = jnp.where((donor == order[0]) | (taker == order[0]) | (lengths[taker] == 0), 0, jnp.maximum(room, 0))
    moved = jax.random.randint(jax.random.fold_in(own, 4), (amount // 2,), 0, 1 << 20) % (room + 1)
    lengths = lengths.at[donor].add(-moved).at[taker].add(moved)
    items = jnp.searchsorted(jnp.cumsum(lengths), jnp.arange(rows * top), side="right").astype(jnp.int32)
    table = items.reshape(top, rows).T
    table = table[jax.random.permutation(jax.random.fold_in(own, 1), rows)]
    turn = jax.random.randint(jax.random.fold_in(own, 2), (rows, 1), 0, top)
    return jnp.take_along_axis(table, (jnp.arange(top)[None, :] + turn) % top, axis=1)


def portions_of(number_of, total, most, slope, full):
    loads = [(1 << 20) // math.isqrt(grade ** slope) + 1 for grade in range(1, number_of + 1)]
    largest = most if full else min(most, max(-(-total // number_of), total * loads[0] // sum(loads)))
    least = 1 if total - largest >= number_of - 1 else 0
    counts, rest = [largest] + [least] * (number_of - 1), total - largest - least * (number_of - 1)
    while rest > 0:
        free = [i for i in range(1, number_of) if counts[i] < largest] or [i for i in range(1, number_of) if counts[i] < most]
        pool, left = sum([loads[i] for i in free]), rest
        for i in free:
            addition = min(most - counts[i], max(1, left * loads[i] // pool), rest)
            counts[i] = counts[i] + addition
            rest = rest - addition
    return np.array(counts)


def normal_values(stream_key, dims, scale, bound, cuts=(), held_as=jnp.bfloat16):
    level = levels(stream_key, dims, cuts, -0.22, 0.18) if cuts else 1.0
    values = jax.random.normal(stream_key, dims, jnp.float32) * scale * level
    return jnp.minimum(jnp.maximum(values, -bound), bound).astype(held_as)


def setup_inputs(seed: int = 0) -> dict:
    key_list = jax.random.split(jax.random.key(seed), 21)
    tokens = normal_values(key_list[0], (BATCH, MODEL_WIDTH), 1.0, 6.0, ((0, 32),))
    state = normal_values(key_list[1], (BATCH, MIXER_HEADS, HEAD_SIZE, HEAD_SIZE), 0.5, 4.0, ((0, 32),), jnp.float32)
    norm_gain = jnp.clip(1.0 + 0.18 * jax.random.normal(key_list[2], (MODEL_WIDTH,), jnp.float32), 0.1, 1.9)
    w_recept = normal_values(key_list[3], (MODEL_WIDTH, MIXER_HEADS * HEAD_SIZE), MODEL_WIDTH ** -0.5, 0.125)
    w_keys = normal_values(key_list[4], (MODEL_WIDTH, MIXER_HEADS * HEAD_SIZE), MODEL_WIDTH ** -0.5, 0.125)
    w_values = normal_values(key_list[5], (MODEL_WIDTH, MIXER_HEADS * HEAD_SIZE), MODEL_WIDTH ** -0.5, 0.125)
    decay_base = normal_values(key_list[6], (MIXER_HEADS * HEAD_SIZE,), 1.0, 3.0, (), jnp.float32)
    decay_first_matrix = normal_values(key_list[7], (MODEL_WIDTH, LOWRANK_WIDTH), MODEL_WIDTH ** -0.5, 0.125)
    decay_second_matrix = normal_values(key_list[8], (LOWRANK_WIDTH, MIXER_HEADS * HEAD_SIZE), LOWRANK_WIDTH ** -0.5, 0.5)
    rate_base = normal_values(key_list[9], (MIXER_HEADS * HEAD_SIZE,), 1.0, 3.0, (), jnp.float32)
    rate_first_matrix = normal_values(key_list[10], (MODEL_WIDTH, LOWRANK_WIDTH), MODEL_WIDTH ** -0.5, 0.125)
    rate_second_matrix = normal_values(key_list[11], (LOWRANK_WIDTH, MIXER_HEADS * HEAD_SIZE), LOWRANK_WIDTH ** -0.5, 0.5)
    head_gain = jnp.clip(1.0 + 0.18 * jax.random.normal(key_list[12], (MIXER_HEADS * HEAD_SIZE,), jnp.float32), 0.1, 1.9)
    w_output = normal_values(key_list[13], (MIXER_HEADS * HEAD_SIZE, MODEL_WIDTH), (MIXER_HEADS * HEAD_SIZE) ** -0.5, 0.1875)
    second_gain = jnp.clip(1.0 + 0.18 * jax.random.normal(key_list[14], (MODEL_WIDTH,), jnp.float32), 0.1, 1.9)
    route_ids_keys = jax.random.split(jax.random.fold_in(key_list[15], 1), BATCH // SEQ_DEV)
    route_ids_turns = jax.random.permutation(jax.random.fold_in(key_list[15], 3), BATCH // SEQ_DEV)
    route_ids = jax.vmap(lambda own, number: assign_block(jax.random.fold_in(key_list[15], 2), own, number, SEQ_DEV, EXPERTS, TOPK, CAP_DEV, 2))(route_ids_keys, route_ids_turns).reshape((BATCH, TOPK))
    route_weights = jnp.clip(jax.random.uniform(key_list[16], (BATCH, TOPK), jnp.float32, 0.2, 1.0), 0.2, 1.0)
    expert_gate = normal_values(key_list[17], (MODEL_WIDTH, EXPERTS * FF_E), MODEL_WIDTH ** -0.5, 0.125, ((1, 32),))
    expert_up = normal_values(key_list[18], (MODEL_WIDTH, EXPERTS * FF_E), MODEL_WIDTH ** -0.5, 0.125, ((1, 32),))
    expert_down = normal_values(key_list[19], (EXPERTS * FF_E, MODEL_WIDTH), FF_E ** -0.5, 0.109375, ((0, 32),))
    return {"tokens": tokens, "state": state, "norm_gain": norm_gain, "w_recept": w_recept, "w_keys": w_keys, "w_values": w_values, "decay_base": decay_base, "decay_first_matrix": decay_first_matrix, "decay_second_matrix": decay_second_matrix, "rate_base": rate_base, "rate_first_matrix": rate_first_matrix, "rate_second_matrix": rate_second_matrix, "head_gain": head_gain, "w_output": w_output, "second_gain": second_gain, "route_ids": route_ids, "route_weights": route_weights, "expert_gate": expert_gate, "expert_up": expert_up, "expert_down": expert_down}


def norm_rows(values, gain):
    mean_sq = lax.optimization_barrier(jnp.mean(values * values, axis=-1, keepdims=True))
    return values * lax.rsqrt(mean_sq + 1e-06) * gain

def time_mixer(tokens, state, norm_gain, w_recept, w_keys, w_values, decay_base, decay_first_matrix, decay_second_matrix, rate_base, rate_first_matrix, rate_second_matrix, head_gain, w_output):
    count = tokens.shape[0]
    heads = state.shape[1]
    width = state.shape[2]
    resid = tokens.astype(jnp.float32)
    normed = norm_rows(resid, norm_gain).astype(jnp.bfloat16)
    recept = jnp.dot(normed, w_recept, preferred_element_type=jnp.float32).astype(jnp.bfloat16)
    keys = jnp.dot(normed, w_keys, preferred_element_type=jnp.float32).astype(jnp.bfloat16)
    vals = jnp.dot(normed, w_values, preferred_element_type=jnp.float32).astype(jnp.bfloat16)
    decay_low = jnp.tanh(jnp.dot(normed, decay_first_matrix, preferred_element_type=jnp.float32)).astype(jnp.bfloat16)
    rate_low = jnp.dot(normed, rate_first_matrix, preferred_element_type=jnp.float32).astype(jnp.bfloat16)
    pre = decay_base + jnp.dot(decay_low, decay_second_matrix, preferred_element_type=jnp.float32)
    decay = jnp.exp(-jnp.exp(-jax.nn.softplus(-pre) - 0.5))
    rate = jax.nn.sigmoid(rate_base + jnp.dot(rate_low, rate_second_matrix, preferred_element_type=jnp.float32))

    def split_heads(values):
        return values.astype(jnp.float32).reshape(count, heads, width)
    r_head = split_heads(recept)
    k_head = split_heads(keys)
    v_head = split_heads(vals)
    d_head = split_heads(decay)
    a_head = split_heads(rate)
    unit = k_head * lax.rsqrt(lax.optimization_barrier(jnp.sum(k_head * k_head, axis=-1, keepdims=True)) + 1e-06)
    probe = jnp.einsum('bhvk,bhk->bhv', state, unit, precision=lax.Precision.HIGHEST)
    updated = state * d_head[:, :, None, :] - probe[..., None] * (unit * a_head)[:, :, None, :] + v_head[..., None] * k_head[:, :, None, :]
    mixed = jnp.einsum('bhvk,bhk->bhv', updated, r_head, precision=lax.Precision.HIGHEST)
    centre = mixed - lax.optimization_barrier(jnp.mean(mixed, axis=-1, keepdims=True))
    spread = lax.optimization_barrier(jnp.mean(centre * centre, axis=-1, keepdims=True))
    mixed = centre * lax.rsqrt(spread + 0.00064)
    mixed = (mixed.reshape(count, heads * width) * head_gain).astype(jnp.bfloat16)
    after = resid + jnp.dot(mixed, w_output, preferred_element_type=jnp.float32)
    return (after, updated)

def expert_part(rows, gate_w, up_w, down_w):
    gate = jnp.dot(rows, gate_w, preferred_element_type=jnp.float32)
    upper = jnp.dot(rows, up_w, preferred_element_type=jnp.float32)
    hidden = (jax.nn.silu(gate) * upper).astype(jnp.bfloat16)
    return jnp.dot(hidden, down_w, preferred_element_type=jnp.float32)

def reference(tokens, state, norm_gain, w_recept, w_keys, w_values, decay_base, decay_first_matrix, decay_second_matrix, rate_base, rate_first_matrix, rate_second_matrix, head_gain, w_output, second_gain, route_ids, route_weights, expert_gate, expert_up, expert_down):
    blocks_tok = tokens.reshape(N_EP, SEQ_DEV, MODEL_WIDTH)
    blocks_state = state.reshape((N_EP, SEQ_DEV) + state.shape[1:])

    def one_block(pair):
        return time_mixer(pair[0], pair[1], norm_gain, w_recept, w_keys, w_values, decay_base, decay_first_matrix, decay_second_matrix, rate_base, rate_first_matrix, rate_second_matrix, head_gain, w_output)
    after, new_state = lax.map(one_block, (blocks_tok, blocks_state))
    after = after.reshape(BATCH, MODEL_WIDTH)
    new_state = new_state.reshape(state.shape)
    second = norm_rows(after, second_gain).astype(jnp.bfloat16)
    gates_all = expert_gate.reshape(MODEL_WIDTH, EXPERTS, FF_E).transpose(1, 0, 2)
    ups_all = expert_up.reshape(MODEL_WIDTH, EXPERTS, FF_E).transpose(1, 0, 2)
    downs_all = expert_down.reshape(EXPERTS, FF_E, MODEL_WIDTH)
    limit = N_EP * CAP_DEV

    def one_expert(total, inputs):
        which, gate_w, up_w, down_w = inputs
        hit = route_ids == which
        member = jnp.any(hit, axis=1)
        share = lax.optimization_barrier(jnp.sum(jnp.where(hit, route_weights, 0.0), axis=1))
        picked = jnp.nonzero(member, size=limit, fill_value=0)[0].astype(jnp.int32)
        valid = (jnp.arange(limit, dtype=jnp.int32) < jnp.sum(member.astype(jnp.int32))).astype(jnp.float32)
        result = expert_part(second[picked], gate_w, up_w, down_w)
        total = total.at[picked].add((share[picked] * valid)[:, None] * result)
        return (total, None)
    blend, _ = lax.scan(one_expert, jnp.zeros((BATCH, MODEL_WIDTH), jnp.float32), (jnp.arange(EXPERTS, dtype=jnp.int32), gates_all, ups_all, downs_all))
    layer_out = (after + blend).astype(jnp.bfloat16)
    return (layer_out, new_state)
```

```python
import functools
import math

import jax
import jax.numpy as jnp
import numpy as np
from jax import lax
from jax.experimental import pallas as pl
from jax.experimental.pallas import tpu as pltpu
from jax.sharding import PartitionSpec as P

EXPERTS = 16
CAP_DEV = 6
ROWS = 8
PARTS = 3
LANES = 128
STRIDE = 32
MIX_CHUNKS = 2
OUT_CHUNKS = 4
MESH = pl.DeviceIdType.MESH
BF = jnp.bfloat16
F32 = jnp.float32


def dot(a, b):
    return jnp.dot(a, b, preferred_element_type=F32)


def split(values):
    high = values.astype(BF)
    return high, (values - high.astype(F32)).astype(BF)


def layer_kernel(
    devices,
    tokens, norm_gain, decay_base, rate_base, head_gain, second_gain, ids, shares, unpack_m, pack_m,
    state, w_recept, w_keys, w_values, d_first, d_second, r_first, r_second, w_output,
    gate_h, up_h, down_h,
    st, ret_out, after_ref, blend_ref,
    wr, wk, wv, df, ds, rf, rs, wo, gate, up, down,
    table, rowbuf, dh, w2, turned, pq, pv, mixed_ref,
    tok_send, tok_buf, mix_send, mix_buf, own_rows, rows_x, hidden,
    part_f, part_b, peer_b, zsend, ret,
    w_sem, in_sem, tsend, trecv, msend, mrecv, xsend, xrecv, ysend, yrecv, rsend, rrecv,
):
    heads, count, width, _ = st.shape
    model = tokens.shape[1]
    inner_mix = heads * width
    group = devices // EXPERTS
    me = lax.axis_index("ep")
    mine = lax.div(me, group)
    place = lax.rem(me, group)
    packed_rows = EXPERTS * ROWS
    rows = EXPERTS * CAP_DEV

    order_of = [
        (d_first, df), (r_first, rf), (w_keys, wk), (w_values, wv), (d_second, ds),
        (r_second, rs), (w_recept, wr), (w_output, wo), (gate_h, gate), (up_h, up), (down_h, down),
    ]
    loads = [
        pltpu.make_async_copy(src, dst, w_sem.at[i]) for i, (src, dst) in enumerate(order_of)
    ]
    for i in (0, 1, 2, 3):
        loads[i].start()

    def other(i):
        total = 0
        for k in range(EXPERTS.bit_length() - 1):
            a = lax.rem(lax.div(mine, 1 << k), 2)
            b = lax.rem(lax.div(i, 1 << k), 2)
            total = total + (a + b - 2 * a * b) * (1 << k)
        return total

    def each_other(body):
        def step(j, c):
            body(other(EXPERTS - j))
            return c

        lax.fori_loop(1, EXPERTS, step, 0)

    def peer(i):
        return lax.rem(place + i, group)

    barrier = pltpu.get_barrier_semaphore()

    def greet(e):
        pl.semaphore_signal(barrier, inc=1, device_id=(e * group + place,), device_id_type=MESH)

    each_other(greet)
    for i in range(1, group):
        pl.semaphore_signal(
            barrier, inc=1, device_id=(mine * group + peer(i),), device_id_type=MESH
        )

    def fetch(h):
        return pltpu.make_async_copy(state.at[:, h], st.at[h], in_sem.at[h])

    def start_fetches(low, high):
        def step(h, c):
            fetch(h).start()
            return c

        lax.fori_loop(low, high, step, 0)

    total_rows = ids.shape[1]
    spot = lax.broadcasted_iota(jnp.int32, (total_rows, count), 0)
    column = lax.broadcasted_iota(jnp.int32, (total_rows, count), 1)
    choose = jnp.where(spot == column + me * count, 1.0, 0.0).astype(BF)
    my_ids = dot(ids[...].astype(F32).astype(BF), choose)
    share_high, share_low = split(shares[...])
    my_shares = dot(share_high, choose) + dot(share_low, choose)
    expert_at = lax.broadcasted_iota(jnp.int32, (EXPERTS, count), 0).astype(F32)
    member = jnp.zeros((EXPERTS, count), F32)
    share = jnp.zeros((EXPERTS, count), F32)
    for k in range(ids.shape[0]):
        hit = jnp.where(expert_at == my_ids[k:k + 1], 1.0, 0.0)
        member = member + hit
        share = share + hit * my_shares[k:k + 1]
    earlier = jnp.where(
        lax.broadcasted_iota(jnp.int32, (count, count), 0)
        < lax.broadcasted_iota(jnp.int32, (count, count), 1),
        1.0, 0.0,
    ).astype(BF)
    order = jnp.where(member > 0.5, dot(member.astype(BF), earlier), -1.0)
    shape = (EXPERTS, ROWS, count)
    slot = jnp.broadcast_to(order[:, None, :], shape)
    weight = jnp.broadcast_to(share[:, None, :], shape)
    at = lax.broadcasted_iota(jnp.int32, shape, 1).astype(F32)
    for j in range(PARTS + 1):
        if j == PARTS:
            hits = (slot == at) & (at < CAP_DEV)
        else:
            hits = (slot == (at - CAP_DEV) * PARTS + j) & (at >= CAP_DEV)
        hits = jnp.where(hits, 1.0, 0.0)
        blend_ref[j] = (hits * weight).reshape(packed_rows, count)
        table[j] = hits.reshape(packed_rows, count).astype(BF)

    def pack(values, put):
        part = values.shape[1] // (PARTS + 1)
        last = values[:, PARTS * part:]
        for j in range(PARTS):
            value = dot(table[PARTS], values[:, j * part:(j + 1) * part]) + dot(table[j], last)
            put(slice(j * part, (j + 1) * part), value.reshape(EXPERTS, ROWS, part).astype(BF))

    def put_tokens(cols, value):
        tok_send[:, :, cols] = value

    pack(tokens[...], put_tokens)
    tok_buf[mine] = tok_send[mine]

    def give_tokens(e):
        return pltpu.make_async_remote_copy(
            src_ref=tok_send.at[e], dst_ref=tok_buf.at[mine],
            send_sem=tsend.at[e], recv_sem=trecv.at[mine],
            device_id=(e * group + place,), device_id_type=MESH,
        )

    def take_tokens(s):
        return pltpu.make_async_remote_copy(
            src_ref=tok_send.at[s], dst_ref=tok_buf.at[s],
            send_sem=tsend.at[s], recv_sem=trecv.at[s],
            device_id=(s * group + place,), device_id_type=MESH,
        )

    pl.semaphore_wait(barrier, EXPERTS - 1 + group - 1)
    each_other(lambda e: give_tokens(e).start())

    resid = tokens[...].astype(F32)
    mean_sq = jnp.mean(resid * resid, axis=-1, keepdims=True)
    normed = (resid * lax.rsqrt(mean_sq + 1e-06) * norm_gain[...]).astype(BF)
    loads[0].wait()
    decay_low = jnp.tanh(dot(normed, df[...])).astype(BF)
    loads[1].wait()
    rate_low = dot(normed, rf[...]).astype(BF)
    loads[2].wait()
    k = dot(normed, wk[...]).astype(BF).astype(F32)
    for i in (4, 5, 6):
        loads[i].start()
    loads[3].wait()
    v = dot(normed, wv[...]).astype(BF).astype(F32)
    start_fetches(0, heads // 2)
    loads[4].wait()
    pre = decay_base[...] + dot(decay_low, ds[...])
    d = jnp.exp(-jax.nn.sigmoid(pre) * math.exp(-0.5))
    loads[5].wait()
    a = jax.nn.sigmoid(rate_base[...] + dot(rate_low, rs[...]))
    loads[6].wait()
    start_fetches(heads // 2, heads)
    r = dot(normed, wr[...]).astype(BF).astype(F32)

    same_head = (
        lax.broadcasted_iota(jnp.int32, (LANES, LANES), 0) // width
        == lax.broadcasted_iota(jnp.int32, (LANES, LANES), 1) // width
    )

    def head_sums(values, scale):
        ones = jnp.where(same_head, scale, 0.0).astype(BF)
        high, low = split(values)
        tiles = [slice(t, t + LANES) for t in range(0, values.shape[1], LANES)]
        return jnp.concatenate([dot(high[:, t], ones) + dot(low[:, t], ones) for t in tiles], axis=1)

    sums = head_sums(jnp.concatenate([k * k, k * a * r, k * r], axis=0), 1.0)
    scale = lax.rsqrt(sums[:count] + 1e-06)
    unit = k * scale
    toward = d * r - unit * (sums[count:2 * count] * scale)
    rowbuf[0] = d
    rowbuf[1] = -unit * a
    rowbuf[2] = k
    rowbuf[3] = v * sums[2 * count:]
    gap = jnp.zeros((STRIDE - count, inner_mix), F32)
    tall = jnp.concatenate(
        [unit, gap, toward, gap, jnp.zeros((STRIDE, inner_mix), F32), v, gap], axis=0
    )
    turned[...] = tall.T.astype(BF)

    block = math.gcd(count, 8)
    lane = lax.broadcasted_iota(jnp.int32, (width, LANES), 1)
    lane_of = lax.rem(lane, STRIDE)

    def first_pass(h, c):
        fetch(h).wait()
        span = pl.ds(pl.multiple_of(h * width, width), width)
        right = turned[span, :]
        acc = jnp.zeros((width, LANES), F32)
        for g in range(count // block):
            s = st[h, g * block:(g + 1) * block]
            got = dot(s.reshape(block * width, width).astype(BF), right)
            got = got.reshape(block, width, LANES)
            for i in range(block):
                acc = jnp.where(lane_of == g * block + i, got[i], acc)
        pq[span, :] = acc
        pv[span, :] = jnp.where(lane < STRIDE, acc, right.astype(F32))
        return c

    wide = inner_mix // MIX_CHUNKS
    half = heads // MIX_CHUNKS

    def give_mixed(n, e):
        return pltpu.make_async_remote_copy(
            src_ref=mix_send.at[n, e], dst_ref=mix_buf.at[n, mine],
            send_sem=msend.at[n, e], recv_sem=mrecv.at[n, mine],
            device_id=(e * group + place,), device_id_type=MESH,
        )

    def take_mixed(n, s):
        return pltpu.make_async_remote_copy(
            src_ref=mix_send.at[n, s], dst_ref=mix_buf.at[n, s],
            send_sem=msend.at[n, s], recv_sem=mrecv.at[n, s],
            device_id=(s * group + place,), device_id_type=MESH,
        )

    def mix_chunk(n):
        lax.fori_loop(n * half, (n + 1) * half, first_pass, 0)
        cols = slice(n * wide, (n + 1) * wide)
        mixed = pq[cols, :].T[STRIDE:STRIDE + count] + rowbuf[3, :, cols]
        centre = mixed - head_sums(mixed, 1.0 / width)
        var = head_sums(centre * centre, 1.0 / width)
        out = (centre * lax.rsqrt(var + 0.00064) * head_gain[:, cols]).astype(BF)
        mixed_ref[:, cols] = out

        def put(at_cols, value):
            mix_send[n, :, :, at_cols] = value

        pack(out, put)
        mix_buf[n, mine] = mix_send[n, mine]
        each_other(lambda e: give_mixed(n, e).start())

    def unpack(source, m, width_of):
        part = width_of // (PARTS + 1)
        pieces, tail = [], jnp.zeros((rows, part), F32)
        for j in range(PARTS):
            value = source(slice(j * part, (j + 1) * part))
            value = value.astype(F32).reshape(packed_rows, part).astype(BF)
            pieces.append(dot(m[PARTS], value))
            tail = tail + dot(m[j], value)
        return pieces + [tail]

    mix_chunk(0)
    loads[7].start()
    loads[8].start()
    mix_chunk(1)
    loads[9].start()
    loads[10].start()

    each_other(lambda s: take_tokens(s).wait_recv())
    for j, piece in enumerate(unpack(lambda cols: tok_buf[:, :, cols], unpack_m, model)):
        part = model // (PARTS + 1)
        own_rows[:, j * part:(j + 1) * part] = piece

    for h in range(heads):
        cols = slice(h * width, (h + 1) * width)
        dh[h] = rowbuf[0, :, cols]
        w2[h] = jnp.concatenate(
            [
                rowbuf[1, :, cols], jnp.zeros((3 * STRIDE - count, width), F32),
                rowbuf[2, :, cols], jnp.zeros((STRIDE - count, width), F32),
            ],
            axis=0,
        ).astype(BF)

    def second_pass(h, c):
        span = pl.ds(pl.multiple_of(h * width, width), width)
        left = pv[span, :]
        right = w2[h]
        decay = dh[h]
        for g in range(count // block):
            some = range(g * block, (g + 1) * block)
            masked = jnp.concatenate([jnp.where(lane_of == b, left, 0.0) for b in some], axis=0)
            change = dot(masked.astype(BF), right).reshape(block, width, width)
            by = jnp.stack([jnp.broadcast_to(decay[b:b + 1], (width, width)) for b in some])
            st[h, g * block:(g + 1) * block] = st[h, g * block:(g + 1) * block] * by + change
        return c

    lax.fori_loop(0, heads, second_pass, 0)

    loads[7].wait()
    step_out = math.gcd(model, 256)

    def add_mixed(n):
        each_other(lambda s: take_mixed(n, s).wait_recv())
        pieces = unpack(lambda cols: mix_buf[n, :, :, cols], unpack_m, wide)
        got = jnp.concatenate(pieces, axis=1).astype(BF)

        def step(t, c):
            cols = pl.ds(pl.multiple_of(t * step_out, step_out), step_out)
            own_rows[:, cols] = own_rows[:, cols] + dot(got, wo[n * wide:(n + 1) * wide, cols])
            return c

        lax.fori_loop(0, model // step_out, step, 0)

    for n in range(MIX_CHUNKS):
        add_mixed(n)

    def second_norm(values):
        mean_of = jnp.mean(values * values, axis=-1, keepdims=True)
        return (values * lax.rsqrt(mean_of + 1e-06) * second_gain[...]).astype(BF)

    rows_x[place] = second_norm(own_rows[...])

    def share_rows(i):
        return pltpu.make_async_remote_copy(
            src_ref=rows_x.at[place], dst_ref=rows_x.at[place],
            send_sem=xsend.at[peer(i)], recv_sem=xrecv.at[place],
            device_id=(mine * group + peer(i),), device_id_type=MESH,
        )

    def shared_rows(i):
        return pltpu.make_async_remote_copy(
            src_ref=rows_x.at[peer(i)], dst_ref=rows_x.at[peer(i)],
            send_sem=xsend.at[peer(i)], recv_sem=xrecv.at[peer(i)],
            device_id=(mine * group + peer(i),), device_id_type=MESH,
        )

    for i in range(1, group):
        share_rows(i).start()

    def after_step(t, c):
        cols = pl.ds(pl.multiple_of(t * step_out, step_out), step_out)
        after_ref[:, cols] = tokens[:, cols].astype(F32) + dot(mixed_ref[...], wo[:, cols])
        return c

    lax.fori_loop(0, model // step_out, after_step, 0)
    loads[8].wait()
    loads[9].wait()
    for i in range(1, group):
        shared_rows(i).wait_recv()

    inner = gate.shape[1]
    step_in = math.gcd(inner, 256)

    def up_step(t, c):
        cols = pl.ds(pl.multiple_of(t * step_in, step_in), step_in)
        left = rows_x[...].reshape(group * rows, model)
        g = dot(left, gate[:, cols])
        u = dot(left, up[:, cols])
        hidden[:, cols] = (g * jax.nn.sigmoid(g) * u).astype(BF)
        return c

    lax.fori_loop(0, inner // step_in, up_step, 0)
    loads[10].wait()
    chunk = model // OUT_CHUNKS
    small = math.gcd(chunk, 256)

    def swap(n, i):
        q = peer(i)
        return pltpu.make_async_remote_copy(
            src_ref=part_b.at[n, q], dst_ref=peer_b.at[n, place],
            send_sem=ysend.at[n, q], recv_sem=yrecv.at[n, place],
            device_id=(mine * group + q,), device_id_type=MESH,
        )

    def swapped(n, i):
        q = peer(i)
        return pltpu.make_async_remote_copy(
            src_ref=part_b.at[n, q], dst_ref=peer_b.at[n, q],
            send_sem=ysend.at[n, q], recv_sem=yrecv.at[n, q],
            device_id=(mine * group + q,), device_id_type=MESH,
        )

    def down_chunk(n, c):
        for t in range(chunk // small):
            cols = pl.ds(pl.multiple_of(n * chunk + t * small, small), small)
            y = dot(hidden[...], down[:, cols])
            for q in range(group):
                piece = y[q * rows:(q + 1) * rows]
                part_f[n, q, :, t * small:(t + 1) * small] = piece
                part_b[n, q, :, t * small:(t + 1) * small] = piece.astype(BF)
        for i in range(1, group):
            swap(n, i).start()
        return c

    lax.fori_loop(0, OUT_CHUNKS, down_chunk, 0)

    def give(n, e):
        return pltpu.make_async_remote_copy(
            src_ref=zsend.at[n, e], dst_ref=ret.at[n, mine],
            send_sem=rsend.at[n, e], recv_sem=rrecv.at[n, mine],
            device_id=(e * group + place,), device_id_type=MESH,
        )

    def take(n, s):
        return pltpu.make_async_remote_copy(
            src_ref=zsend.at[n, s], dst_ref=ret.at[n, s],
            send_sem=rsend.at[n, s], recv_sem=rrecv.at[n, s],
            device_id=(s * group + place,), device_id_type=MESH,
        )

    part = chunk // (PARTS + 1)

    def return_chunk(n, c):
        for i in range(1, group):
            swapped(n, i).wait_recv()

        def summed(cols):
            total = part_f[n, place, :, cols]
            for i in range(1, group):
                total = total + peer_b[n, peer(i), :, cols].astype(F32)
            return total.astype(BF)

        last = summed(slice(PARTS * part, chunk))
        for j in range(PARTS):
            cols = slice(j * part, (j + 1) * part)
            value = dot(pack_m[PARTS], summed(cols)) + dot(pack_m[j], last)
            zsend[n, :, :, cols] = value.reshape(EXPERTS, ROWS, part).astype(BF)
        ret[n, mine] = zsend[n, mine]
        each_other(lambda e: give(n, e).start())
        return c

    lax.fori_loop(0, OUT_CHUNKS, return_chunk, 0)

    def end_sends(e):
        give_tokens(e).wait_send()
        for n in range(MIX_CHUNKS):
            give_mixed(n, e).wait_send()

    each_other(end_sends)
    for i in range(1, group):
        share_rows(i).wait_send()

    def end_chunk(n, c):
        for i in range(1, group):
            swap(n, i).wait_send()
        each_other(lambda s: take(n, s).wait_recv())
        ret_out[n] = ret[n]
        return c

    lax.fori_loop(0, OUT_CHUNKS, end_chunk, 0)

    def end_give(n, c):
        each_other(lambda e: give(n, e).wait_send())
        return c

    lax.fori_loop(0, OUT_CHUNKS, end_give, 0)


def finish_kernel(st, ret, after, blend_w, new_state, layer_out, out, sem, out_sem):
    heads = st.shape[0]

    def put(h):
        return pltpu.make_async_copy(st.at[h], new_state.at[:, h], sem.at[h])

    def start(h, c):
        put(h).start()
        return c

    lax.fori_loop(0, heads, start, 0)

    def dot_turned(left, right):
        return lax.dot_general(left, right, (((0,), (0,)), ((), ())), preferred_element_type=F32)

    high, low = split(blend_w[...])
    chunk = after.shape[1] // OUT_CHUNKS
    part = chunk // (PARTS + 1)
    packed_rows = EXPERTS * ROWS
    for n in range(OUT_CHUNKS):
        tail_at = slice(n * chunk + PARTS * part, (n + 1) * chunk)
        tail = after[:, tail_at]
        for j in range(PARTS):
            cols = slice(n * chunk + j * part, n * chunk + (j + 1) * part)
            block = ret[n, :, :, j * part:(j + 1) * part]
            block = block.astype(F32).reshape(packed_rows, part).astype(BF)
            value = after[:, cols] + dot_turned(high[PARTS], block) + dot_turned(low[PARTS], block)
            out[:, cols] = value.astype(BF)
            tail = tail + dot_turned(high[j], block) + dot_turned(low[j], block)
        out[:, tail_at] = tail.astype(BF)
    last = pltpu.make_async_copy(out, layer_out, out_sem.at[0])
    last.start()

    def end(h, c):
        put(h).wait()
        return c

    lax.fori_loop(0, heads, end, 0)
    last.wait()


def maps():
    rows = EXPERTS * CAP_DEV
    row = np.arange(rows)[:, None]
    place = np.arange(EXPERTS * ROWS)[None, :]
    same = row // CAP_DEV == place // ROWS
    slot, at = row % CAP_DEV, place % ROWS
    found = [
        same & (at == CAP_DEV + slot // PARTS) & (slot % PARTS == j) for j in range(PARTS)
    ] + [same & (at == slot)]
    found = np.stack(found).astype(np.float32)
    return jnp.asarray(found, BF), jnp.asarray(found.transpose(0, 2, 1), BF)


def on_device(
    tokens, state, norm_gain, w_recept, w_keys, w_values, decay_base, decay_first_matrix,
    decay_second_matrix, rate_base, rate_first_matrix, rate_second_matrix, head_gain, w_output,
    second_gain, route_ids, route_weights, expert_gate, expert_up, expert_down,
):
    devices = lax.axis_size("ep")
    group = devices // EXPERTS
    count, heads, width, _ = state.shape
    model = tokens.shape[1]
    inner = expert_gate.shape[1]
    mix = heads * width
    rows = EXPERTS * CAP_DEV
    packed_rows = EXPERTS * ROWS
    folded = PARTS * model // (PARTS + 1)
    mix_fold = PARTS * (mix // MIX_CHUNKS) // (PARTS + 1)
    out_fold = PARTS * (model // OUT_CHUNKS) // (PARTS + 1)
    unpack_m, pack_m = maps()
    vm = pl.BlockSpec(memory_space=pltpu.VMEM)
    hb = pl.BlockSpec(memory_space=pl.ANY)
    dma = pltpu.SemaphoreType.DMA
    weights = [
        w_recept, w_keys, w_values, decay_first_matrix, decay_second_matrix, rate_first_matrix,
        rate_second_matrix, w_output, expert_gate, expert_up, expert_down,
    ]
    st, ret, after, blend_w = pl.pallas_call(
        functools.partial(layer_kernel, devices),
        out_shape=(
            pltpu.VMEM((heads, count, width, width), F32),
            pltpu.VMEM((OUT_CHUNKS, EXPERTS, ROWS, out_fold), BF),
            pltpu.VMEM((count, model), F32),
            pltpu.VMEM((PARTS + 1, packed_rows, count), F32),
        ),
        in_specs=[vm] * 10 + [hb] * 12,
        out_specs=(vm, vm, vm, vm),
        scratch_shapes=[
            *[pltpu.VMEM(w.shape, BF) for w in weights],
            pltpu.VMEM((PARTS + 1, packed_rows, count), BF),
            pltpu.VMEM((4, count, mix), F32),
            pltpu.VMEM((heads, count, width), F32),
            pltpu.VMEM((heads, LANES, width), BF),
            pltpu.VMEM((mix, LANES), BF),
            pltpu.VMEM((mix, LANES), F32),
            pltpu.VMEM((mix, LANES), F32),
            pltpu.VMEM((count, mix), BF),
            pltpu.VMEM((EXPERTS, ROWS, folded), BF),
            pltpu.VMEM((EXPERTS, ROWS, folded), BF),
            pltpu.VMEM((MIX_CHUNKS, EXPERTS, ROWS, mix_fold), BF),
            pltpu.VMEM((MIX_CHUNKS, EXPERTS, ROWS, mix_fold), BF),
            pltpu.VMEM((rows, model), F32),
            pltpu.VMEM((group, rows, model), BF),
            pltpu.VMEM((group * rows, inner), BF),
            pltpu.VMEM((OUT_CHUNKS, group, rows, model // OUT_CHUNKS), F32),
            pltpu.VMEM((OUT_CHUNKS, group, rows, model // OUT_CHUNKS), BF),
            pltpu.VMEM((OUT_CHUNKS, group, rows, model // OUT_CHUNKS), BF),
            pltpu.VMEM((OUT_CHUNKS, EXPERTS, ROWS, out_fold), BF),
            pltpu.VMEM((OUT_CHUNKS, EXPERTS, ROWS, out_fold), BF),
            dma((len(weights),)),
            dma((heads,)),
            dma((EXPERTS,)),
            dma((EXPERTS,)),
            dma((MIX_CHUNKS, EXPERTS)),
            dma((MIX_CHUNKS, EXPERTS)),
            dma((group,)),
            dma((group,)),
            dma((OUT_CHUNKS, group)),
            dma((OUT_CHUNKS, group)),
            dma((OUT_CHUNKS, EXPERTS)),
            dma((OUT_CHUNKS, EXPERTS)),
        ],
        compiler_params=pltpu.CompilerParams(
            collective_id=0, has_side_effects=True, vmem_limit_bytes=49 * 1024 * 1024
        ),
        name="layer",
    )(
        tokens, norm_gain[None], decay_base[None], rate_base[None], head_gain[None],
        second_gain[None], route_ids.T, route_weights.T, unpack_m, pack_m, state, w_recept, w_keys,
        w_values, decay_first_matrix, decay_second_matrix, rate_first_matrix, rate_second_matrix,
        w_output, expert_gate, expert_up, expert_down,
    )
    new_state, layer_out = pl.pallas_call(
        finish_kernel,
        out_shape=(
            jax.ShapeDtypeStruct(state.shape, F32),
            jax.ShapeDtypeStruct((count, model), BF),
        ),
        in_specs=[vm] * 4,
        out_specs=(hb, hb),
        scratch_shapes=[pltpu.VMEM((count, model), BF), dma((heads,)), dma((1,))],
        compiler_params=pltpu.CompilerParams(vmem_limit_bytes=4 * 1024 * 1024),
        name="finish",
    )(st, ret, after, blend_w)
    return (layer_out, new_state)


def solution(mesh):
    rep = P()
    in_specs = (
        P("ep", None), P("ep", None, None, None), *[rep] * 15,
        P(None, "ep"), P(None, "ep"), P("ep", None),
    )
    out_specs = (P("ep", None), P("ep", None, None, None))
    return jax.shard_map(
        on_device, mesh=mesh, in_specs=in_specs, out_specs=out_specs, check_vma=False
    )
```

```python
import functools
import math

import jax
import jax.numpy as jnp
import numpy as np
from jax import lax
from jax.experimental import pallas as pl
from jax.experimental.pallas import tpu as pltpu
from jax.sharding import PartitionSpec as P

EXPERTS = 16
CAP_DEV = 6
ROWS = 8
PARTS = 3
LANES = 128
STRIDE = 32
MIX_CHUNKS = 2
OUT_CHUNKS = 4
PAIRS_AT_ONCE = 2
LAG = 3
BESIDE = (8, 4)
MESH = pl.DeviceIdType.MESH
BF = jnp.bfloat16
F32 = jnp.float32


def dot(a, b):
    return jnp.dot(a, b, preferred_element_type=F32)


def split(values):
    high = values.astype(BF)
    return high, (values - high.astype(F32)).astype(BF)


def layer_kernel(
    devices,
    tokens_h, norm_gain_h, decay_base_h, rate_base_h, head_gain_h, second_gain_h, ids_h, shares_h,
    unpack_h, pack_h, state, w_recept, w_keys, w_values, d_first, d_second, r_first, r_second, w_output,
    gate_h, up_h, down_h,
    st, ret_out, after_ref, blend_ref,
    tokens, norm_gain, decay_base, rate_base, head_gain, second_gain, ids, shares, unpack_m, pack_m,
    wr, wk, wv, df, ds, rf, rs, wo, gate, up, down,
    far_tokens, table, rowbuf, dh, w2, turned, v_turned, pq, pv, mixed_ref,
    tok_send, tok_buf, mix_send, mix_buf, own_rows, rows_x, hidden,
    part_f, part_b, peer_b, zsend, ret,
    s_sem, w_sem, in_sem, gsend, grecv, tsend, trecv, msend, mrecv, xsend, xrecv, ysend, yrecv, rsend, rrecv,
):
    heads, count, width, _ = st.shape
    model = tokens.shape[1]
    inner_mix = heads * width
    group = devices // EXPERTS
    me = lax.axis_index("ep")
    mine = lax.div(me, group)
    place = lax.rem(me, group)
    packed_rows = EXPERTS * ROWS
    rows = EXPERTS * CAP_DEV

    wide = inner_mix // MIX_CHUNKS
    half = heads // MIX_CHUNKS

    def load(i, src, dst):
        return pltpu.make_async_copy(src, dst, w_sem.at[i])

    def load_columns(i, n, src, dst):
        cols = pl.ds(n * wide, wide)
        return load(i, src.at[:, cols], dst.at[:, cols])

    low_loads = [
        load(i, src, dst)
        for i, (src, dst) in enumerate([(d_first, df), (r_first, rf), (d_second, ds), (r_second, rs)])
    ]
    mix_loads = [
        [
            load_columns(4 + 3 * n + i, n, src, dst)
            for i, (src, dst) in enumerate([(w_keys, wk), (w_values, wv), (w_recept, wr)])
        ]
        for n in range(MIX_CHUNKS)
    ]
    late = 4 + 3 * MIX_CHUNKS
    out_load, gate_load, up_load, down_load = [
        load(late + i, src, dst)
        for i, (src, dst) in enumerate([(w_output, wo), (gate_h, gate), (up_h, up), (down_h, down)])
    ]
    small_of = [
        (ids_h, ids), (shares_h, shares), (tokens_h, tokens), (norm_gain_h, norm_gain),
        (decay_base_h, decay_base), (rate_base_h, rate_base), (head_gain_h, head_gain),
        (second_gain_h, second_gain), (unpack_h, unpack_m), (pack_h, pack_m),
    ]
    smalls = [
        pltpu.make_async_copy(src, dst, s_sem.at[i]) for i, (src, dst) in enumerate(small_of)
    ]
    for copy in smalls:
        copy.start()
    for copy in low_loads + mix_loads[0]:
        copy.start()
    def fetch(h):
        return pltpu.make_async_copy(state.at[:, h], st.at[h], in_sem.at[h])

    def start_fetches(low, high):
        def step(h, c):
            fetch(h).start()
            return c

        lax.fori_loop(low, high, step, 0)

    start_fetches(0, half)
    for copy in mix_loads[1]:
        copy.start()
    start_fetches(half, heads)


    def other(i):
        total = 0
        for k in range(EXPERTS.bit_length() - 1):
            a = lax.rem(lax.div(mine, 1 << k), 2)
            b = lax.rem(lax.div(i, 1 << k), 2)
            total = total + (a + b - 2 * a * b) * (1 << k)
        return total

    others = [other(i) for i in range(EXPERTS - 1, 0, -1)]

    def each_other(body):
        for e in others:
            body(e)

    def peer(i):
        return lax.rem(place + i, group)

    barrier = pltpu.get_barrier_semaphore()

    def greet(e):
        pl.semaphore_signal(barrier, inc=1, device_id=(e * group + place,), device_id_type=MESH)

    each_other(greet)
    for i in range(1, group):
        pl.semaphore_signal(
            barrier, inc=1, device_id=(mine * group + peer(i),), device_id_type=MESH
        )

    for i in (0, 1, 2):
        smalls[i].wait()
    total_rows = ids.shape[1]
    spot = lax.broadcasted_iota(jnp.int32, (total_rows, count), 0)
    column = lax.broadcasted_iota(jnp.int32, (total_rows, count), 1)
    all_ids = ids[...].astype(F32).astype(BF)
    choose = jnp.where(spot == column + me * count, 1.0, 0.0).astype(BF)
    share_high, share_low = split(shares[...])
    my_shares = dot(share_high, choose) + dot(share_low, choose)
    expert_at = lax.broadcasted_iota(jnp.int32, (EXPERTS, count), 0).astype(F32)
    earlier = jnp.where(
        lax.broadcasted_iota(jnp.int32, (count, count), 0)
        < lax.broadcasted_iota(jnp.int32, (count, count), 1),
        1.0, 0.0,
    ).astype(BF)
    shape = (EXPERTS, ROWS, count)
    at = lax.broadcasted_iota(jnp.int32, shape, 1).astype(F32)

    def slots(chosen):
        ids_of = dot(all_ids, chosen)
        hits = [
            jnp.where(expert_at == ids_of[i:i + 1], 1.0, 0.0) for i in range(ids.shape[0])
        ]
        member = functools.reduce(jnp.add, hits)
        order = jnp.where(member > 0.5, dot(member.astype(BF), earlier), -1.0)
        slot = jnp.broadcast_to(order[:, None, :], shape)
        found = [
            (slot == (at - CAP_DEV) * PARTS + j) & (at >= CAP_DEV) for j in range(PARTS)
        ] + [(slot == at) & (at < CAP_DEV)]
        return hits, [jnp.where(f, 1.0, 0.0) for f in found]

    hits, found = slots(choose)
    share = functools.reduce(
        jnp.add, [hit * my_shares[i:i + 1] for i, hit in enumerate(hits)]
    )
    weight = jnp.broadcast_to(share[:, None, :], shape)
    for j in range(PARTS + 1):
        blend_ref[j] = (found[j] * weight).reshape(packed_rows, count)
        table[0, j] = found[j].reshape(packed_rows, count).astype(BF)

    def pack(which, values, put):
        part = values.shape[1] // (PARTS + 1)
        last = values[:, PARTS * part:]
        for j in range(PARTS):
            value = dot(table[which, PARTS], values[:, j * part:(j + 1) * part])
            value = value + dot(table[which, j], last)
            put(slice(j * part, (j + 1) * part), value.reshape(EXPERTS, ROWS, part).astype(BF))

    def put_tokens(which):
        def put(cols, value):
            tok_send[which, :, :, cols] = value

        return put

    far = other(EXPERTS // 2)
    far_device = far * group + place
    near = others[EXPERTS // 2:]

    def give_whole():
        return pltpu.make_async_remote_copy(
            src_ref=tokens, dst_ref=far_tokens, send_sem=gsend, recv_sem=grecv,
            device_id=(far_device,), device_id_type=MESH,
        )

    def give_tokens(which, e):
        return pltpu.make_async_remote_copy(
            src_ref=tok_send.at[which, e], dst_ref=tok_buf.at[far if which else mine],
            send_sem=tsend, recv_sem=trecv,
            device_id=(e * group + place,), device_id_type=MESH,
        )

    rest = pl.ds(0, EXPERTS - 1)

    def all_tokens():
        some = pl.ds(0, EXPERTS - 2)
        return pltpu.make_async_remote_copy(
            src_ref=tok_buf.at[some], dst_ref=tok_buf.at[some],
            send_sem=tsend, recv_sem=trecv,
            device_id=(others[0] * group + place,), device_id_type=MESH,
        )

    pl.semaphore_wait(barrier, EXPERTS - 1 + group - 1)
    give_whole().start()
    pack(0, tokens[...], put_tokens(0))
    for e in near:
        give_tokens(0, e).start()
    tok_buf[mine] = tok_send[0, mine]

    _, found = slots(jnp.where(spot == column + far_device * count, 1.0, 0.0).astype(BF))
    for j in range(PARTS + 1):
        table[1, j] = found[j].reshape(packed_rows, count).astype(BF)

    for i in range(3, len(smalls)):
        smalls[i].wait()
    resid = tokens[...].astype(F32)
    mean_sq = jnp.mean(resid * resid, axis=-1, keepdims=True)
    normed = (resid * lax.rsqrt(mean_sq + 1e-06) * norm_gain[...]).astype(BF)
    low_loads[0].wait()
    decay_low = jnp.tanh(dot(normed, df[...])).astype(BF)
    low_loads[1].wait()
    rate_low = dot(normed, rf[...]).astype(BF)
    low_loads[2].wait()
    low_loads[3].wait()

    same_head = (
        lax.broadcasted_iota(jnp.int32, (LANES, LANES), 0) // width
        == lax.broadcasted_iota(jnp.int32, (LANES, LANES), 1) // width
    )

    def head_sums(values, scale):
        ones = jnp.where(same_head, scale, 0.0).astype(BF)
        high, low = split(values)
        tiles = [slice(t, t + LANES) for t in range(0, values.shape[1], LANES)]
        return jnp.concatenate([dot(high[:, t], ones) + dot(low[:, t], ones) for t in tiles], axis=1)

    gap = jnp.zeros((STRIDE - count, wide), F32)

    side = lax.broadcasted_iota(jnp.int32, (wide, LANES), 1) // width
    own_side = lax.rem(lax.broadcasted_iota(jnp.int32, (wide, LANES), 0) // width, 2) == side

    def project(n):
        cols = slice(n * wide, (n + 1) * wide)
        pre = decay_base[:, cols] + dot(decay_low, ds[:, cols])
        d = jnp.exp(-jax.nn.sigmoid(pre) * math.exp(-0.5))
        a = jax.nn.sigmoid(rate_base[:, cols] + dot(rate_low, rs[:, cols]))
        if n == 0:
            mix_loads[0][0].wait()
        k = dot(normed, wk[:, cols]).astype(BF).astype(F32)
        if n == 0:
            mix_loads[0][1].wait()
        v = dot(normed, wv[:, cols]).astype(BF).astype(F32)
        if n == 0:
            mix_loads[0][2].wait()
        r = dot(normed, wr[:, cols]).astype(BF).astype(F32)
        sums = head_sums(jnp.concatenate([k * k, k * a * r, k * r], axis=0), 1.0)
        scale = lax.rsqrt(sums[:count] + 1e-06)
        unit = k * scale
        toward = d * r - unit * (sums[count:2 * count] * scale)
        rowbuf[0, :, cols] = d
        rowbuf[1, :, cols] = -unit * a
        rowbuf[2, :, cols] = k
        rowbuf[3, :, cols] = v * sums[2 * count:]
        tall = jnp.concatenate([unit, gap, toward, gap] * 2, axis=0)
        turned[cols, :] = jnp.where(own_side, tall.T, 0.0).astype(BF)
        tall = jnp.concatenate([jnp.zeros((STRIDE, wide), F32), v, gap] * 2, axis=0)
        v_turned[cols, :] = jnp.where(own_side, tall.T, 0.0)

    block = math.gcd(count, 8)
    lane = lax.broadcasted_iota(jnp.int32, (width, LANES), 1)
    lane_of = lax.rem(lane, STRIDE)

    def pairs(body, low, high):
        def step(t, c):
            for i in range(PAIRS_AT_ONCE):
                body(t * PAIRS_AT_ONCE + i)
            return c

        lax.fori_loop(low // PAIRS_AT_ONCE, high // PAIRS_AT_ONCE, step, 0)

    def first_pass(p):
        for i in range(2):
            fetch(2 * p + i).wait()
        span = pl.ds(pl.multiple_of(2 * p * width, 2 * width), 2 * width)
        right = turned[span, :]
        acc = jnp.zeros((width, LANES), F32)
        for g in range(count // block):
            some = [
                st[2 * p + i, g * block:(g + 1) * block].reshape(block * width, width).astype(BF)
                for i in range(2)
            ]
            got = dot(jnp.concatenate(some, axis=1), right).reshape(block, width, LANES)
            for i in range(block):
                acc = jnp.where(lane_of == g * block + i, got[i], acc)
        v_both = v_turned[span, :]
        v_both = v_both[:width] + v_both[width:]
        span = pl.ds(pl.multiple_of(p * width, width), width)
        pq[span, :] = acc
        pv[span, :] = jnp.where(lax.rem(lane, 2 * STRIDE) < STRIDE, acc, v_both)

    def give_mixed(n, e):
        return pltpu.make_async_remote_copy(
            src_ref=mix_send.at[n, e], dst_ref=mix_buf.at[n, mine],
            send_sem=msend.at[n], recv_sem=mrecv.at[n],
            device_id=(e * group + place,), device_id_type=MESH,
        )

    def all_mixed(n):
        return pltpu.make_async_remote_copy(
            src_ref=mix_send.at[n, rest], dst_ref=mix_buf.at[n, rest],
            send_sem=msend.at[n], recv_sem=mrecv.at[n],
            device_id=(others[0] * group + place,), device_id_type=MESH,
        )

    def mix_chunk(n):
        cols = slice(n * wide, (n + 1) * wide)
        both = pq[n * wide // 2:(n + 1) * wide // 2, :].T
        even, odd = both[STRIDE:STRIDE + count], both[3 * STRIDE:3 * STRIDE + count]
        low = lax.broadcasted_iota(jnp.int32, (count, LANES), 1) < width
        tiles = []
        for t in range(0, wide // 2, LANES):
            e, o = even[:, t:t + LANES], odd[:, t:t + LANES]
            tiles.append(jnp.where(low, e, pltpu.roll(o, width, axis=1)))
            tiles.append(jnp.where(low, pltpu.roll(e, width, axis=1), o))
        mixed = jnp.concatenate(tiles, axis=1) + rowbuf[3, :, cols]
        centre = mixed - head_sums(mixed, 1.0 / width)
        var = head_sums(centre * centre, 1.0 / width)
        out = (centre * lax.rsqrt(var + 0.00064) * head_gain[:, cols]).astype(BF)
        mixed_ref[:, cols] = out

        def put(at_cols, value):
            mix_send[n, :, :, at_cols] = value

        pack(0, out, put)
        mix_buf[n, mine] = mix_send[n, mine]

    def send_chunk(n):
        each_other(lambda e: give_mixed(n, e).start())

    batch = rows // 2
    my_half = lax.div(mine, EXPERTS // 2)
    halves = [1 - my_half, my_half]
    spans = [pl.ds(pl.multiple_of(h * batch, 16), batch) for h in halves]
    blocks = [pl.ds(h * (EXPERTS // 2), EXPERTS // 2) for h in halves]

    def unpack(source, width_of):
        part = width_of // (PARTS + 1)
        pieces, tail = [], jnp.zeros((batch, part), F32)
        for j in range(PARTS):
            value = source(slice(j * part, (j + 1) * part))
            value = value.astype(F32).reshape(packed_rows // 2, part).astype(BF)
            pieces.append(dot(unpack_m[PARTS], value))
            tail = tail + dot(unpack_m[j], value)
        return pieces + [tail]

    project(0)
    pairs(first_pass, 0, half // 2)
    for copy in mix_loads[1]:
        copy.wait()
    mix_chunk(0)
    project(1)
    send_chunk(0)
    give_whole().wait_recv()
    pack(1, far_tokens[...], put_tokens(1))
    tok_buf[far] = tok_send[1, mine]
    for e in near:
        give_tokens(1, e).start()
    pairs(first_pass, half // 2, half // 2 + half // 4)
    out_load.start()
    gate_load.start()
    pairs(first_pass, half // 2 + half // 4, half)
    mix_chunk(1)
    send_chunk(1)
    up_load.start()
    down_load.start()

    for h in range(heads):
        cols = slice(h * width, (h + 1) * width)
        dh[h] = rowbuf[0, :, cols]
        lines = [
            rowbuf[1, :, cols], jnp.zeros((STRIDE - count, width), F32),
            rowbuf[2, :, cols], jnp.zeros((STRIDE - count, width), F32),
        ]
        blank = [jnp.zeros((2 * STRIDE, width), F32)]
        lines = lines + blank if h % 2 == 0 else blank + lines
        w2[h] = jnp.concatenate(lines, axis=0).astype(BF)

    def second_pass(p):
        left = pv[pl.ds(pl.multiple_of(p * width, width), width), :]
        for g in range(count // block):
            some = range(g * block, (g + 1) * block)
            masked = jnp.concatenate([jnp.where(lane_of == b, left, 0.0) for b in some], axis=0)
            masked = masked.astype(BF)
            for i in range(2):
                h = 2 * p + i
                decay = dh[h]
                change = dot(masked, w2[h]).reshape(block, width, width)
                by = jnp.stack([jnp.broadcast_to(decay[b:b + 1], (width, width)) for b in some])
                st[h, g * block:(g + 1) * block] = st[h, g * block:(g + 1) * block] * by + change

    first_pairs = BESIDE[0] * heads // 32
    next_pairs = first_pairs + BESIDE[1] * heads // 32
    pairs(second_pass, 0, first_pairs)
    all_tokens().wait_recv()
    for b in range(2):
        for j, piece in enumerate(unpack(lambda cols: tok_buf[blocks[b], :, cols], model)):
            part = model // (PARTS + 1)
            own_rows[spans[b], j * part:(j + 1) * part] = piece
    out_load.wait()
    step_out = math.gcd(model, 256)

    def add_mixed(n, b):
        pieces = unpack(lambda cols: mix_buf[n, blocks[b], :, cols], wide)
        got = jnp.concatenate(pieces, axis=1).astype(BF)
        for t in range(model // step_out):
            cols = slice(t * step_out, (t + 1) * step_out)
            more = dot(got, wo[n * wide:(n + 1) * wide, cols])
            own_rows[spans[b], cols] = own_rows[spans[b], cols] + more

    for n in range(MIX_CHUNKS - 1):
        all_mixed(n).wait_recv()
        for b in range(2):
            add_mixed(n, b)
    all_mixed(MIX_CHUNKS - 1).wait_recv()

    def second_norm(values):
        mean_of = jnp.mean(values * values, axis=-1, keepdims=True)
        return (values * lax.rsqrt(mean_of + 1e-06) * second_gain[...]).astype(BF)

    def share_rows(b, i):
        return pltpu.make_async_remote_copy(
            src_ref=rows_x.at[place, spans[b]], dst_ref=rows_x.at[place, spans[b]],
            send_sem=xsend.at[b, peer(i)], recv_sem=xrecv.at[b, place],
            device_id=(mine * group + peer(i),), device_id_type=MESH,
        )

    def shared_rows(b, i):
        return pltpu.make_async_remote_copy(
            src_ref=rows_x.at[peer(i), spans[b]], dst_ref=rows_x.at[peer(i), spans[b]],
            send_sem=xsend.at[b, peer(i)], recv_sem=xrecv.at[b, peer(i)],
            device_id=(mine * group + peer(i),), device_id_type=MESH,
        )

    for b in range(2):
        add_mixed(MIX_CHUNKS - 1, b)
        rows_x[place, spans[b]] = second_norm(own_rows[spans[b], :])
        for i in range(1, group):
            share_rows(b, i).start()
    pairs(second_pass, first_pairs, next_pairs)
    gate_load.wait()
    up_load.wait()

    inner = gate.shape[1]
    step_in = math.gcd(inner, 256)

    chunk = model // OUT_CHUNKS
    small = math.gcd(chunk, 256)
    part = chunk // (PARTS + 1)
    low_mine = lax.rem(mine, EXPERTS // 2)
    targets = [
        [halves[0] * (EXPERTS // 2) + i for i in range(EXPERTS // 2)],
        [
            my_half * (EXPERTS // 2) + i + jnp.where(low_mine <= i, 1, 0)
            for i in range(EXPERTS // 2 - 1)
        ],
    ]

    def expand(b, low, high):
        left = jnp.concatenate([rows_x[q, spans[b], :] for q in range(group)], axis=0)
        for t in range(low, high):
            cols = slice(t * step_in, (t + 1) * step_in)
            g = dot(left, gate[:, cols])
            u = dot(left, up[:, cols])
            hidden[:, cols] = (g * jax.nn.sigmoid(g) * u).astype(BF)

    def swap(b, n, i):
        q = peer(i)
        return pltpu.make_async_remote_copy(
            src_ref=part_b.at[n, q, spans[b]], dst_ref=peer_b.at[n, place, spans[b]],
            send_sem=ysend.at[b, n, q], recv_sem=yrecv.at[b, n, place],
            device_id=(mine * group + q,), device_id_type=MESH,
        )

    def swapped(b, n, i):
        q = peer(i)
        return pltpu.make_async_remote_copy(
            src_ref=part_b.at[n, q, spans[b]], dst_ref=peer_b.at[n, q, spans[b]],
            send_sem=ysend.at[b, n, q], recv_sem=yrecv.at[b, n, q],
            device_id=(mine * group + q,), device_id_type=MESH,
        )

    def down_chunk(b, n):
        for t in range(chunk // small):
            cols = slice(n * chunk + t * small, n * chunk + (t + 1) * small)
            y = dot(hidden[...], down[:, cols])
            for q in range(group):
                piece = y[q * batch:(q + 1) * batch]
                part_f[n, q, spans[b], t * small:(t + 1) * small] = piece
                part_b[n, q, spans[b], t * small:(t + 1) * small] = piece.astype(BF)
        for i in range(1, group):
            swap(b, n, i).start()

    def give(n, e):
        return pltpu.make_async_remote_copy(
            src_ref=zsend.at[n, e], dst_ref=ret.at[n, mine],
            send_sem=rsend.at[n], recv_sem=rrecv.at[n],
            device_id=(e * group + place,), device_id_type=MESH,
        )

    def all_given(n):
        return pltpu.make_async_remote_copy(
            src_ref=zsend.at[n, rest], dst_ref=ret.at[n, rest],
            send_sem=rsend.at[n], recv_sem=rrecv.at[n],
            device_id=(others[0] * group + place,), device_id_type=MESH,
        )

    def return_chunk(b, n):
        for i in range(1, group):
            swapped(b, n, i).wait_recv()

        def summed(cols):
            total = part_f[n, place, spans[b], cols]
            for i in range(1, group):
                total = total + peer_b[n, peer(i), spans[b], cols].astype(F32)
            return total.astype(BF)

        last = summed(slice(PARTS * part, chunk))
        for j in range(PARTS):
            cols = slice(j * part, (j + 1) * part)
            value = dot(pack_m[PARTS], summed(cols)) + dot(pack_m[j], last)
            zsend[n, blocks[b], :, cols] = value.reshape(EXPERTS // 2, ROWS, part).astype(BF)
        for e in targets[b]:
            give(n, e).start()
        if b == 1:
            ret[n, mine] = zsend[n, mine]

    def rows_here(b):
        for i in range(1, group):
            shared_rows(b, i).wait_recv()

    steps = inner // step_in
    rows_here(0)
    expand(0, 0, steps)
    down_load.wait()
    for n in range(OUT_CHUNKS):
        down_chunk(0, n)
        if n >= LAG:
            return_chunk(0, n - LAG)
    rows_here(1)
    for n in range(OUT_CHUNKS - LAG, OUT_CHUNKS - 1):
        return_chunk(0, n)
    expand(1, 0, steps // 3)
    return_chunk(0, OUT_CHUNKS - 1)
    expand(1, steps // 3, steps)
    for n in range(OUT_CHUNKS):
        down_chunk(1, n)
        if n >= LAG:
            return_chunk(1, n - LAG)
    for n in range(OUT_CHUNKS - LAG, OUT_CHUNKS):
        return_chunk(1, n)

    pairs(second_pass, next_pairs, heads // 2)
    for t in range(model // step_out):
        cols = slice(t * step_out, (t + 1) * step_out)
        after_ref[:, cols] = tokens[:, cols].astype(F32) + dot(mixed_ref[...], wo[:, cols])

    give_whole().wait_send()
    all_tokens().wait_send()
    for n in range(MIX_CHUNKS):
        all_mixed(n).wait_send()
    for i in range(1, group):
        for b in range(2):
            share_rows(b, i).wait_send()
            for n in range(OUT_CHUNKS):
                swap(b, n, i).wait_send()
    for n in range(OUT_CHUNKS):
        all_given(n).wait_recv()
        ret_out[n] = ret[n]
    for n in range(OUT_CHUNKS):
        all_given(n).wait_send()


def finish_kernel(st, ret, after, blend_w, new_state, layer_out, out, sem, out_sem):
    heads = st.shape[0]

    def put(h):
        return pltpu.make_async_copy(st.at[h], new_state.at[:, h], sem.at[h])

    def start(h, c):
        put(h).start()
        return c

    lax.fori_loop(0, heads, start, 0)

    def dot_turned(left, right):
        return lax.dot_general(left, right, (((0,), (0,)), ((), ())), preferred_element_type=F32)

    high, low = split(blend_w[...])
    chunk = after.shape[1] // OUT_CHUNKS
    part = chunk // (PARTS + 1)
    packed_rows = EXPERTS * ROWS
    for n in range(OUT_CHUNKS):
        tail_at = slice(n * chunk + PARTS * part, (n + 1) * chunk)
        tail = after[:, tail_at]
        for j in range(PARTS):
            cols = slice(n * chunk + j * part, n * chunk + (j + 1) * part)
            block = ret[n, :, :, j * part:(j + 1) * part]
            block = block.astype(F32).reshape(packed_rows, part).astype(BF)
            value = after[:, cols] + dot_turned(high[PARTS], block) + dot_turned(low[PARTS], block)
            out[:, cols] = value.astype(BF)
            tail = tail + dot_turned(high[j], block) + dot_turned(low[j], block)
        out[:, tail_at] = tail.astype(BF)
    last = pltpu.make_async_copy(out, layer_out, out_sem.at[0])
    last.start()

    def end(h, c):
        put(h).wait()
        return c

    lax.fori_loop(0, heads, end, 0)
    last.wait()


def maps(experts):
    rows = experts * CAP_DEV
    row = np.arange(rows)[:, None]
    place = np.arange(experts * ROWS)[None, :]
    same = row // CAP_DEV == place // ROWS
    slot, at = row % CAP_DEV, place % ROWS
    found = [
        same & (at == CAP_DEV + slot // PARTS) & (slot % PARTS == j) for j in range(PARTS)
    ] + [same & (at == slot)]
    found = np.stack(found).astype(np.float32)
    return jnp.asarray(found, BF), jnp.asarray(found.transpose(0, 2, 1), BF)


def on_device(
    tokens, state, norm_gain, w_recept, w_keys, w_values, decay_base, decay_first_matrix,
    decay_second_matrix, rate_base, rate_first_matrix, rate_second_matrix, head_gain, w_output,
    second_gain, route_ids, route_weights, expert_gate, expert_up, expert_down,
):
    devices = lax.axis_size("ep")
    group = devices // EXPERTS
    count, heads, width, _ = state.shape
    model = tokens.shape[1]
    inner = expert_gate.shape[1]
    mix = heads * width
    rows = EXPERTS * CAP_DEV
    packed_rows = EXPERTS * ROWS
    folded = PARTS * model // (PARTS + 1)
    mix_fold = PARTS * (mix // MIX_CHUNKS) // (PARTS + 1)
    out_fold = PARTS * (model // OUT_CHUNKS) // (PARTS + 1)
    unpack_m, pack_m = maps(EXPERTS // 2)
    vm = pl.BlockSpec(memory_space=pltpu.VMEM)
    hb = pl.BlockSpec(memory_space=pl.ANY)
    dma = pltpu.SemaphoreType.DMA
    weights = [
        w_recept, w_keys, w_values, decay_first_matrix, decay_second_matrix, rate_first_matrix,
        rate_second_matrix, w_output, expert_gate, expert_up, expert_down,
    ]
    smalls = [
        tokens, norm_gain[None], decay_base[None], rate_base[None], head_gain[None],
        second_gain[None], route_ids.T, route_weights.T, unpack_m, pack_m,
    ]
    st, ret, after, blend_w = pl.pallas_call(
        functools.partial(layer_kernel, devices),
        out_shape=(
            pltpu.VMEM((heads, count, width, width), F32),
            pltpu.VMEM((OUT_CHUNKS, EXPERTS, ROWS, out_fold), BF),
            pltpu.VMEM((count, model), F32),
            pltpu.VMEM((PARTS + 1, packed_rows, count), F32),
        ),
        in_specs=[hb] * 22,
        out_specs=(vm, vm, vm, vm),
        scratch_shapes=[
            *[pltpu.VMEM(w.shape, w.dtype) for w in smalls],
            *[pltpu.VMEM(w.shape, BF) for w in weights],
            pltpu.VMEM((count, model), BF),
            pltpu.VMEM((2, PARTS + 1, packed_rows, count), BF),
            pltpu.VMEM((4, count, mix), F32),
            pltpu.VMEM((heads, count, width), F32),
            pltpu.VMEM((heads, LANES, width), BF),
            pltpu.VMEM((mix, LANES), BF),
            pltpu.VMEM((mix, LANES), F32),
            pltpu.VMEM((mix // 2, LANES), F32),
            pltpu.VMEM((mix // 2, LANES), F32),
            pltpu.VMEM((count, mix), BF),
            pltpu.VMEM((2, EXPERTS, ROWS, folded), BF),
            pltpu.VMEM((EXPERTS, ROWS, folded), BF),
            pltpu.VMEM((MIX_CHUNKS, EXPERTS, ROWS, mix_fold), BF),
            pltpu.VMEM((MIX_CHUNKS, EXPERTS, ROWS, mix_fold), BF),
            pltpu.VMEM((rows, model), F32),
            pltpu.VMEM((group, rows, model), BF),
            pltpu.VMEM((group * rows // 2, inner), BF),
            pltpu.VMEM((OUT_CHUNKS, group, rows, model // OUT_CHUNKS), F32),
            pltpu.VMEM((OUT_CHUNKS, group, rows, model // OUT_CHUNKS), BF),
            pltpu.VMEM((OUT_CHUNKS, group, rows, model // OUT_CHUNKS), BF),
            pltpu.VMEM((OUT_CHUNKS, EXPERTS, ROWS, out_fold), BF),
            pltpu.VMEM((OUT_CHUNKS, EXPERTS, ROWS, out_fold), BF),
            dma((len(smalls),)),
            dma((8 + 3 * MIX_CHUNKS,)),
            dma((heads,)),
            dma,
            dma,
            dma,
            dma,
            dma((MIX_CHUNKS,)),
            dma((MIX_CHUNKS,)),
            dma((2, group)),
            dma((2, group)),
            dma((2, OUT_CHUNKS, group)),
            dma((2, OUT_CHUNKS, group)),
            dma((OUT_CHUNKS,)),
            dma((OUT_CHUNKS,)),
        ],
        compiler_params=pltpu.CompilerParams(
            collective_id=0, has_side_effects=True, vmem_limit_bytes=49 * 1024 * 1024
        ),
        name="layer",
    )(
        *smalls, state, w_recept, w_keys, w_values, decay_first_matrix, decay_second_matrix, rate_first_matrix, rate_second_matrix,
        w_output, expert_gate, expert_up, expert_down,
    )
    new_state, layer_out = pl.pallas_call(
        finish_kernel,
        out_shape=(
            jax.ShapeDtypeStruct(state.shape, F32),
            jax.ShapeDtypeStruct((count, model), BF),
        ),
        in_specs=[vm] * 4,
        out_specs=(hb, hb),
        scratch_shapes=[pltpu.VMEM((count, model), BF), dma((heads,)), dma((1,))],
        compiler_params=pltpu.CompilerParams(vmem_limit_bytes=4 * 1024 * 1024),
        name="finish",
    )(st, ret, after, blend_w)
    return (layer_out, new_state)


def solution(mesh):
    rep = P()
    in_specs = (
        P("ep", None), P("ep", None, None, None), *[rep] * 15,
        P(None, "ep"), P(None, "ep"), P("ep", None),
    )
    out_specs = (P("ep", None), P("ep", None, None, None))
    return jax.shard_map(
        on_device, mesh=mesh, in_specs=in_specs, out_specs=out_specs, check_vma=False
    )
```

```python
import functools
import math

import jax
import jax.numpy as jnp
import numpy as np
from jax import lax
from jax.experimental import pallas as pl
from jax.experimental.pallas import tpu as pltpu
from jax.sharding import PartitionSpec as P

EXPERTS = 16
CAP_DEV = 6
ROWS = 8
PARTS = 3
LANES = 128
STRIDE = 32
MIX_CHUNKS = 2
OUT_CHUNKS = 4
PAIRS_AT_ONCE = 2
LAG = 3
URGENT = 1
BESIDE = (8, 4)
MESH = pl.DeviceIdType.MESH
BF = jnp.bfloat16
F32 = jnp.float32


def dot(a, b):
    return jnp.dot(a, b, preferred_element_type=F32)


def split(values):
    high = values.astype(BF)
    return high, (values - high.astype(F32)).astype(BF)


def layer_kernel(
    devices,
    tokens_h, norm_gain_h, decay_base_h, rate_base_h, head_gain_h, second_gain_h, ids_h, shares_h,
    unpack_h, pack_h, state, w_recept, w_keys, w_values, d_first, d_second, r_first, r_second, w_output,
    gate_h, up_h, down_h,
    st, ret_out, after_ref, blend_ref,
    tokens, norm_gain, decay_base, rate_base, head_gain, second_gain, ids, shares, unpack_m, pack_m,
    wr, wk, wv, df, ds, rf, rs, wo, gate, up, down,
    far_tokens, table, rowbuf, dh, w2, turned, v_turned, pq, pv, mixed_ref,
    tok_send, tok_buf, mix_send, mix_buf, own_rows, rows_x, hidden,
    part_f, part_b, peer_b, zsend, ret,
    s_sem, w_sem, in_sem, gsend, grecv, tsend, trecv, msend, mrecv, xsend, xrecv, ysend, yrecv, rsend, rrecv,
):
    heads, count, width, _ = st.shape
    model = tokens.shape[1]
    inner_mix = heads * width
    group = devices // EXPERTS
    me = lax.axis_index("ep")
    mine = lax.div(me, group)
    place = lax.rem(me, group)
    packed_rows = EXPERTS * ROWS
    rows = EXPERTS * CAP_DEV

    def other(i):
        total = 0
        for k in range(EXPERTS.bit_length() - 1):
            a = lax.rem(lax.div(mine, 1 << k), 2)
            b = lax.rem(lax.div(i, 1 << k), 2)
            total = total + (a + b - 2 * a * b) * (1 << k)
        return total

    others = [other(i) for i in range(EXPERTS - 1, 0, -1)]

    def each_other(body):
        for e in others:
            body(e)

    def peer(i):
        return lax.rem(place + i, group)

    barrier = pltpu.get_barrier_semaphore()

    def greet(e):
        pl.semaphore_signal(barrier, inc=1, device_id=(e * group + place,), device_id_type=MESH)

    each_other(greet)
    for i in range(1, group):
        pl.semaphore_signal(
            barrier, inc=1, device_id=(mine * group + peer(i),), device_id_type=MESH
        )

    wide = inner_mix // MIX_CHUNKS
    half = heads // MIX_CHUNKS

    def load(i, src, dst):
        return pltpu.make_async_copy(src, dst, w_sem.at[i])

    def load_columns(i, n, src, dst):
        cols = pl.ds(n * wide, wide)
        return load(i, src.at[:, cols], dst.at[:, cols])

    low_loads = [
        load(i, src, dst)
        for i, (src, dst) in enumerate([(d_first, df), (r_first, rf), (d_second, ds), (r_second, rs)])
    ]
    mix_loads = [
        [
            load_columns(4 + 3 * n + i, n, src, dst)
            for i, (src, dst) in enumerate([(w_keys, wk), (w_values, wv), (w_recept, wr)])
        ]
        for n in range(MIX_CHUNKS)
    ]
    late = 4 + 3 * MIX_CHUNKS
    out_load, gate_load, up_load, down_load = [
        load(late + i, src, dst)
        for i, (src, dst) in enumerate([(w_output, wo), (gate_h, gate), (up_h, up), (down_h, down)])
    ]
    small_of = [
        (ids_h, ids), (shares_h, shares), (tokens_h, tokens), (norm_gain_h, norm_gain),
        (decay_base_h, decay_base), (rate_base_h, rate_base), (head_gain_h, head_gain),
        (second_gain_h, second_gain), (unpack_h, unpack_m), (pack_h, pack_m),
    ]
    smalls = [
        pltpu.make_async_copy(src, dst, s_sem.at[i]) for i, (src, dst) in enumerate(small_of)
    ]
    for copy in smalls:
        copy.start()
    for copy in low_loads + mix_loads[0]:
        copy.start()
    def fetch(h):
        return pltpu.make_async_copy(state.at[:, h], st.at[h], in_sem.at[h])

    def start_fetches(low, high):
        def step(h, c):
            fetch(h).start()
            return c

        lax.fori_loop(low, high, step, 0)

    start_fetches(0, half)
    for copy in mix_loads[1]:
        copy.start()
    start_fetches(half, heads)


    for i in (0, 1, 2):
        smalls[i].wait()
    total_rows = ids.shape[1]
    spot = lax.broadcasted_iota(jnp.int32, (total_rows, count), 0)
    column = lax.broadcasted_iota(jnp.int32, (total_rows, count), 1)
    all_ids = ids[...].astype(F32).astype(BF)
    choose = jnp.where(spot == column + me * count, 1.0, 0.0).astype(BF)
    share_high, share_low = split(shares[...])
    my_shares = dot(share_high, choose) + dot(share_low, choose)
    expert_at = lax.broadcasted_iota(jnp.int32, (EXPERTS, count), 0).astype(F32)
    earlier = jnp.where(
        lax.broadcasted_iota(jnp.int32, (count, count), 0)
        < lax.broadcasted_iota(jnp.int32, (count, count), 1),
        1.0, 0.0,
    ).astype(BF)
    shape = (EXPERTS, ROWS, count)
    at = lax.broadcasted_iota(jnp.int32, shape, 1).astype(F32)

    def slots(chosen):
        ids_of = dot(all_ids, chosen)
        hits = [
            jnp.where(expert_at == ids_of[i:i + 1], 1.0, 0.0) for i in range(ids.shape[0])
        ]
        member = functools.reduce(jnp.add, hits)
        order = jnp.where(member > 0.5, dot(member.astype(BF), earlier), -1.0)
        slot = jnp.broadcast_to(order[:, None, :], shape)
        found = [
            (slot == (at - CAP_DEV) * PARTS + j) & (at >= CAP_DEV) for j in range(PARTS)
        ] + [(slot == at) & (at < CAP_DEV)]
        return hits, [jnp.where(f, 1.0, 0.0) for f in found]

    hits, found = slots(choose)
    share = functools.reduce(
        jnp.add, [hit * my_shares[i:i + 1] for i, hit in enumerate(hits)]
    )
    weight = jnp.broadcast_to(share[:, None, :], shape)
    for j in range(PARTS + 1):
        blend_ref[j] = (found[j] * weight).reshape(packed_rows, count)
        table[0, j] = found[j].reshape(packed_rows, count).astype(BF)

    def pack(which, values, put):
        part = values.shape[1] // (PARTS + 1)
        last = values[:, PARTS * part:]
        for j in range(PARTS):
            value = dot(table[which, PARTS], values[:, j * part:(j + 1) * part])
            value = value + dot(table[which, j], last)
            put(slice(j * part, (j + 1) * part), value.reshape(EXPERTS, ROWS, part).astype(BF))

    def put_tokens(which):
        def put(cols, value):
            tok_send[which, :, :, cols] = value

        return put

    far = other(EXPERTS // 2)
    far_device = far * group + place
    near = others[EXPERTS // 2:]

    def give_whole():
        return pltpu.make_async_remote_copy(
            src_ref=tokens, dst_ref=far_tokens, send_sem=gsend, recv_sem=grecv,
            device_id=(far_device,), device_id_type=MESH,
        )

    def give_tokens(which, e):
        return pltpu.make_async_remote_copy(
            src_ref=tok_send.at[which, e], dst_ref=tok_buf.at[far if which else mine],
            send_sem=tsend, recv_sem=trecv,
            device_id=(e * group + place,), device_id_type=MESH,
        )

    rest = pl.ds(0, EXPERTS - 1)

    def all_tokens():
        some = pl.ds(0, EXPERTS - 2)
        return pltpu.make_async_remote_copy(
            src_ref=tok_buf.at[some], dst_ref=tok_buf.at[some],
            send_sem=tsend, recv_sem=trecv,
            device_id=(others[0] * group + place,), device_id_type=MESH,
        )

    pl.semaphore_wait(barrier, EXPERTS - 1 + group - 1)
    give_whole().start()
    pack(0, tokens[...], put_tokens(0))
    for e in near:
        give_tokens(0, e).start()
    tok_buf[mine] = tok_send[0, mine]

    _, found = slots(jnp.where(spot == column + far_device * count, 1.0, 0.0).astype(BF))
    for j in range(PARTS + 1):
        table[1, j] = found[j].reshape(packed_rows, count).astype(BF)

    for i in range(3, len(smalls)):
        smalls[i].wait()
    resid = tokens[...].astype(F32)
    mean_sq = jnp.mean(resid * resid, axis=-1, keepdims=True)
    normed = (resid * lax.rsqrt(mean_sq + 1e-06) * norm_gain[...]).astype(BF)
    low_loads[0].wait()
    decay_low = jnp.tanh(dot(normed, df[...])).astype(BF)
    low_loads[1].wait()
    rate_low = dot(normed, rf[...]).astype(BF)
    low_loads[2].wait()
    low_loads[3].wait()

    same_head = (
        lax.broadcasted_iota(jnp.int32, (LANES, LANES), 0) // width
        == lax.broadcasted_iota(jnp.int32, (LANES, LANES), 1) // width
    )

    def head_sums(values, scale):
        ones = jnp.where(same_head, scale, 0.0).astype(BF)
        high, low = split(values)
        tiles = [slice(t, t + LANES) for t in range(0, values.shape[1], LANES)]
        return jnp.concatenate([dot(high[:, t], ones) + dot(low[:, t], ones) for t in tiles], axis=1)

    gap = jnp.zeros((STRIDE - count, wide), F32)

    side = lax.broadcasted_iota(jnp.int32, (wide, LANES), 1) // width
    own_side = lax.rem(lax.broadcasted_iota(jnp.int32, (wide, LANES), 0) // width, 2) == side

    def project(n):
        cols = slice(n * wide, (n + 1) * wide)
        pre = decay_base[:, cols] + dot(decay_low, ds[:, cols])
        d = jnp.exp(-jax.nn.sigmoid(pre) * math.exp(-0.5))
        a = jax.nn.sigmoid(rate_base[:, cols] + dot(rate_low, rs[:, cols]))
        if n == 0:
            mix_loads[0][0].wait()
        k = dot(normed, wk[:, cols]).astype(BF).astype(F32)
        if n == 0:
            mix_loads[0][1].wait()
        v = dot(normed, wv[:, cols]).astype(BF).astype(F32)
        if n == 0:
            mix_loads[0][2].wait()
        r = dot(normed, wr[:, cols]).astype(BF).astype(F32)
        sums = head_sums(jnp.concatenate([k * k, k * a * r, k * r], axis=0), 1.0)
        scale = lax.rsqrt(sums[:count] + 1e-06)
        unit = k * scale
        toward = d * r - unit * (sums[count:2 * count] * scale)
        rowbuf[0, :, cols] = d
        rowbuf[1, :, cols] = -unit * a
        rowbuf[2, :, cols] = k
        rowbuf[3, :, cols] = v * sums[2 * count:]
        tall = jnp.concatenate([unit, gap, toward, gap] * 2, axis=0)
        turned[cols, :] = jnp.where(own_side, tall.T, 0.0).astype(BF)
        tall = jnp.concatenate([jnp.zeros((STRIDE, wide), F32), v, gap] * 2, axis=0)
        v_turned[cols, :] = jnp.where(own_side, tall.T, 0.0)

    block = math.gcd(count, 8)
    lane = lax.broadcasted_iota(jnp.int32, (width, LANES), 1)
    lane_of = lax.rem(lane, STRIDE)

    def pairs(body, low, high):
        def step(t, c):
            for i in range(PAIRS_AT_ONCE):
                body(t * PAIRS_AT_ONCE + i)
            return c

        lax.fori_loop(low // PAIRS_AT_ONCE, high // PAIRS_AT_ONCE, step, 0)

    def first_pass(t):
        low = t * PAIRS_AT_ONCE
        for i in range(2 * PAIRS_AT_ONCE):
            fetch(2 * low + i).wait()
        spans_in = [
            pl.ds(pl.multiple_of(2 * (low + i) * width, 2 * width), 2 * width)
            for i in range(PAIRS_AT_ONCE)
        ]
        blank = jnp.zeros((2 * width, LANES), BF)
        right = jnp.concatenate(
            [
                jnp.concatenate(
                    [turned[at, :] if i == j else blank for j in range(PAIRS_AT_ONCE)], axis=1
                )
                for i, at in enumerate(spans_in)
            ],
            axis=0,
        )
        acc = [jnp.zeros((width, LANES), F32) for _ in range(PAIRS_AT_ONCE)]
        for g in range(count // block):
            some = [
                st[2 * low + i, g * block:(g + 1) * block].reshape(block * width, width).astype(BF)
                for i in range(2 * PAIRS_AT_ONCE)
            ]
            got = dot(jnp.concatenate(some, axis=1), right)
            for j in range(PAIRS_AT_ONCE):
                here = got[:, j * LANES:(j + 1) * LANES].reshape(block, width, LANES)
                for i in range(block):
                    acc[j] = jnp.where(lane_of == g * block + i, here[i], acc[j])
        for j in range(PAIRS_AT_ONCE):
            v_both = v_turned[spans_in[j], :]
            v_both = v_both[:width] + v_both[width:]
            span = pl.ds(pl.multiple_of((low + j) * width, width), width)
            pq[span, :] = acc[j]
            pv[span, :] = jnp.where(lax.rem(lane, 2 * STRIDE) < STRIDE, acc[j], v_both)

    def first_passes(low, high):
        def step(t, c):
            first_pass(t)
            return c

        lax.fori_loop(low // PAIRS_AT_ONCE, high // PAIRS_AT_ONCE, step, 0)

    def give_mixed(n, e):
        return pltpu.make_async_remote_copy(
            src_ref=mix_send.at[n, e], dst_ref=mix_buf.at[n, mine],
            send_sem=msend.at[n], recv_sem=mrecv.at[n],
            device_id=(e * group + place,), device_id_type=MESH,
        )

    def all_mixed(n):
        return pltpu.make_async_remote_copy(
            src_ref=mix_send.at[n, rest], dst_ref=mix_buf.at[n, rest],
            send_sem=msend.at[n], recv_sem=mrecv.at[n],
            device_id=(others[0] * group + place,), device_id_type=MESH,
        )

    def mix_chunk(n):
        cols = slice(n * wide, (n + 1) * wide)
        both = pq[n * wide // 2:(n + 1) * wide // 2, :].T
        even, odd = both[STRIDE:STRIDE + count], both[3 * STRIDE:3 * STRIDE + count]
        low = lax.broadcasted_iota(jnp.int32, (count, LANES), 1) < width
        tiles = []
        for t in range(0, wide // 2, LANES):
            e, o = even[:, t:t + LANES], odd[:, t:t + LANES]
            tiles.append(jnp.where(low, e, pltpu.roll(o, width, axis=1)))
            tiles.append(jnp.where(low, pltpu.roll(e, width, axis=1), o))
        mixed = jnp.concatenate(tiles, axis=1) + rowbuf[3, :, cols]
        centre = mixed - head_sums(mixed, 1.0 / width)
        var = head_sums(centre * centre, 1.0 / width)
        out = (centre * lax.rsqrt(var + 0.00064) * head_gain[:, cols]).astype(BF)
        mixed_ref[:, cols] = out

        def put(at_cols, value):
            mix_send[n, :, :, at_cols] = value

        pack(0, out, put)
        mix_buf[n, mine] = mix_send[n, mine]

    def send_chunk(n):
        each_other(lambda e: give_mixed(n, e).start())

    batch = rows // 2
    my_half = lax.div(mine, EXPERTS // 2)
    halves = [1 - my_half, my_half]
    spans = [pl.ds(pl.multiple_of(h * batch, 16), batch) for h in halves]
    blocks = [pl.ds(h * (EXPERTS // 2), EXPERTS // 2) for h in halves]

    def unpack(source, width_of):
        part = width_of // (PARTS + 1)
        pieces, tail = [], jnp.zeros((batch, part), F32)
        for j in range(PARTS):
            value = source(slice(j * part, (j + 1) * part))
            value = value.astype(F32).reshape(packed_rows // 2, part).astype(BF)
            pieces.append(dot(unpack_m[PARTS], value))
            tail = tail + dot(unpack_m[j], value)
        return pieces + [tail]

    project(0)
    first_passes(0, half // 2)
    for copy in mix_loads[1]:
        copy.wait()
    mix_chunk(0)
    project(1)
    send_chunk(0)
    give_whole().wait_recv()
    pack(1, far_tokens[...], put_tokens(1))
    tok_buf[far] = tok_send[1, mine]
    for e in near:
        give_tokens(1, e).start()
    first_passes(half // 2, half // 2 + half // 4)
    out_load.start()
    gate_load.start()
    first_passes(half // 2 + half // 4, half)
    mix_chunk(1)
    send_chunk(1)
    up_load.start()
    down_load.start()

    for h in range(heads):
        cols = slice(h * width, (h + 1) * width)
        dh[h] = rowbuf[0, :, cols]
        lines = [
            rowbuf[1, :, cols], jnp.zeros((STRIDE - count, width), F32),
            rowbuf[2, :, cols], jnp.zeros((STRIDE - count, width), F32),
        ]
        blank = [jnp.zeros((2 * STRIDE, width), F32)]
        lines = lines + blank if h % 2 == 0 else blank + lines
        w2[h] = jnp.concatenate(lines, axis=0).astype(BF)

    def second_pass(p):
        left = pv[pl.ds(pl.multiple_of(p * width, width), width), :]
        for g in range(count // block):
            some = range(g * block, (g + 1) * block)
            masked = jnp.concatenate([jnp.where(lane_of == b, left, 0.0) for b in some], axis=0)
            masked = masked.astype(BF)
            for i in range(2):
                h = 2 * p + i
                decay = dh[h]
                change = dot(masked, w2[h]).reshape(block, width, width)
                by = jnp.stack([jnp.broadcast_to(decay[b:b + 1], (width, width)) for b in some])
                st[h, g * block:(g + 1) * block] = st[h, g * block:(g + 1) * block] * by + change

    first_pairs = BESIDE[0] * heads // 32
    next_pairs = first_pairs + BESIDE[1] * heads // 32
    pairs(second_pass, 0, first_pairs)
    out_load.wait()
    step_out = math.gcd(model, 256)

    def add_mixed(n, b):
        pieces = unpack(lambda cols: mix_buf[n, blocks[b], :, cols], wide)
        got = jnp.concatenate(pieces, axis=1).astype(BF)
        for t in range(model // step_out):
            cols = slice(t * step_out, (t + 1) * step_out)
            more = dot(got, wo[n * wide:(n + 1) * wide, cols])
            own_rows[spans[b], cols] = more if n == 0 else own_rows[spans[b], cols] + more

    for n in range(MIX_CHUNKS - 1):
        all_mixed(n).wait_recv()
        for b in range(2):
            add_mixed(n, b)
    all_tokens().wait_recv()
    for b in range(2):
        for j, piece in enumerate(unpack(lambda cols: tok_buf[blocks[b], :, cols], model)):
            part = model // (PARTS + 1)
            cols = slice(j * part, (j + 1) * part)
            own_rows[spans[b], cols] = own_rows[spans[b], cols] + piece
    all_mixed(MIX_CHUNKS - 1).wait_recv()

    def second_norm(values):
        mean_of = jnp.mean(values * values, axis=-1, keepdims=True)
        return (values * lax.rsqrt(mean_of + 1e-06) * second_gain[...]).astype(BF)

    def share_rows(b, i):
        return pltpu.make_async_remote_copy(
            src_ref=rows_x.at[place, spans[b]], dst_ref=rows_x.at[place, spans[b]],
            send_sem=xsend.at[b, peer(i)], recv_sem=xrecv.at[b, place],
            device_id=(mine * group + peer(i),), device_id_type=MESH,
        )

    def shared_rows(b, i):
        return pltpu.make_async_remote_copy(
            src_ref=rows_x.at[peer(i), spans[b]], dst_ref=rows_x.at[peer(i), spans[b]],
            send_sem=xsend.at[b, peer(i)], recv_sem=xrecv.at[b, peer(i)],
            device_id=(mine * group + peer(i),), device_id_type=MESH,
        )

    for b in range(2):
        add_mixed(MIX_CHUNKS - 1, b)
        rows_x[place, spans[b]] = second_norm(own_rows[spans[b], :])
        for i in range(1, group):
            share_rows(b, i).start()
    pairs(second_pass, first_pairs, next_pairs)
    gate_load.wait()
    up_load.wait()

    inner = gate.shape[1]
    step_in = math.gcd(inner, 256)

    chunk = model // OUT_CHUNKS
    small = math.gcd(chunk, 256)
    part = chunk // (PARTS + 1)
    low_mine = lax.rem(mine, EXPERTS // 2)
    targets = [
        [halves[0] * (EXPERTS // 2) + i for i in range(EXPERTS // 2)],
        [
            my_half * (EXPERTS // 2) + i + jnp.where(low_mine <= i, 1, 0)
            for i in range(EXPERTS // 2 - 1)
        ],
    ]

    def expand(b, low, high):
        left = jnp.concatenate([rows_x[q, spans[b], :] for q in range(group)], axis=0)
        for t in range(low, high):
            cols = slice(t * step_in, (t + 1) * step_in)
            g = dot(left, gate[:, cols])
            u = dot(left, up[:, cols])
            hidden[:, cols] = (g * jax.nn.sigmoid(g) * u).astype(BF)

    def swap(b, n, i):
        q = peer(i)
        return pltpu.make_async_remote_copy(
            src_ref=part_b.at[n, q, spans[b]], dst_ref=peer_b.at[n, place, spans[b]],
            send_sem=ysend.at[b, n, q], recv_sem=yrecv.at[b, n, place],
            device_id=(mine * group + q,), device_id_type=MESH,
        )

    def swapped(b, n, i):
        q = peer(i)
        return pltpu.make_async_remote_copy(
            src_ref=part_b.at[n, q, spans[b]], dst_ref=peer_b.at[n, q, spans[b]],
            send_sem=ysend.at[b, n, q], recv_sem=yrecv.at[b, n, q],
            device_id=(mine * group + q,), device_id_type=MESH,
        )

    def down_chunk(b, n):
        for t in range(chunk // small):
            cols = slice(n * chunk + t * small, n * chunk + (t + 1) * small)
            y = dot(hidden[...], down[:, cols])
            for q in range(group):
                piece = y[q * batch:(q + 1) * batch]
                part_f[n, q, spans[b], t * small:(t + 1) * small] = piece
                part_b[n, q, spans[b], t * small:(t + 1) * small] = piece.astype(BF)
        for i in range(1, group):
            swap(b, n, i).start()

    def give(n, e):
        return pltpu.make_async_remote_copy(
            src_ref=zsend.at[n, e], dst_ref=ret.at[n, mine],
            send_sem=rsend.at[n], recv_sem=rrecv.at[n],
            device_id=(e * group + place,), device_id_type=MESH,
        )

    def all_given(n):
        return pltpu.make_async_remote_copy(
            src_ref=zsend.at[n, rest], dst_ref=ret.at[n, rest],
            send_sem=rsend.at[n], recv_sem=rrecv.at[n],
            device_id=(others[0] * group + place,), device_id_type=MESH,
        )

    def return_chunk(b, n):
        for i in range(1, group):
            swapped(b, n, i).wait_recv()

        def summed(cols):
            total = part_f[n, place, spans[b], cols]
            for i in range(1, group):
                total = total + peer_b[n, peer(i), spans[b], cols].astype(F32)
            return total.astype(BF)

        last = summed(slice(PARTS * part, chunk))
        for j in range(PARTS):
            cols = slice(j * part, (j + 1) * part)
            value = dot(pack_m[PARTS], summed(cols)) + dot(pack_m[j], last)
            zsend[n, blocks[b], :, cols] = value.reshape(EXPERTS // 2, ROWS, part).astype(BF)
        if b == 1:
            for e in targets[1]:
                give(n, e).start()
            ret[n, mine] = zsend[n, mine]
            return
        for e in targets[0][:URGENT]:
            give(n, e).start()
        for m in [n - 1] * (n > 0) + [n] * (n == OUT_CHUNKS - 1):
            for e in targets[0][URGENT:]:
                give(m, e).start()

    def rows_here(b):
        for i in range(1, group):
            shared_rows(b, i).wait_recv()

    steps = inner // step_in
    rows_here(0)
    expand(0, 0, steps)
    down_load.wait()
    for n in range(OUT_CHUNKS):
        down_chunk(0, n)
        if n >= LAG:
            return_chunk(0, n - LAG)
    rows_here(1)
    for n in range(OUT_CHUNKS - LAG, OUT_CHUNKS - 1):
        return_chunk(0, n)
    expand(1, 0, steps // 3)
    return_chunk(0, OUT_CHUNKS - 1)
    expand(1, steps // 3, steps)
    for n in range(OUT_CHUNKS):
        down_chunk(1, n)
        if n >= LAG:
            return_chunk(1, n - LAG)
    for n in range(OUT_CHUNKS - LAG, OUT_CHUNKS):
        return_chunk(1, n)

    pairs(second_pass, next_pairs, heads // 2)
    for t in range(model // step_out):
        cols = slice(t * step_out, (t + 1) * step_out)
        after_ref[:, cols] = tokens[:, cols].astype(F32) + dot(mixed_ref[...], wo[:, cols])

    give_whole().wait_send()
    all_tokens().wait_send()
    for n in range(MIX_CHUNKS):
        all_mixed(n).wait_send()
    for i in range(1, group):
        for b in range(2):
            share_rows(b, i).wait_send()
            for n in range(OUT_CHUNKS):
                swap(b, n, i).wait_send()
    for n in range(OUT_CHUNKS):
        all_given(n).wait_recv()
        ret_out[n] = ret[n]
    for n in range(OUT_CHUNKS):
        all_given(n).wait_send()


def finish_kernel(st, ret, after, blend_w, new_state, layer_out, out, sem, out_sem):
    heads = st.shape[0]

    def put(h):
        return pltpu.make_async_copy(st.at[h], new_state.at[:, h], sem.at[h])

    def start(h, c):
        put(h).start()
        return c

    lax.fori_loop(0, heads, start, 0)

    def dot_turned(left, right):
        return lax.dot_general(left, right, (((0,), (0,)), ((), ())), preferred_element_type=F32)

    high, low = split(blend_w[...])
    chunk = after.shape[1] // OUT_CHUNKS
    part = chunk // (PARTS + 1)
    packed_rows = EXPERTS * ROWS
    for n in range(OUT_CHUNKS):
        tail_at = slice(n * chunk + PARTS * part, (n + 1) * chunk)
        tail = after[:, tail_at]
        for j in range(PARTS):
            cols = slice(n * chunk + j * part, n * chunk + (j + 1) * part)
            block = ret[n, :, :, j * part:(j + 1) * part]
            block = block.astype(F32).reshape(packed_rows, part).astype(BF)
            value = after[:, cols] + dot_turned(high[PARTS], block) + dot_turned(low[PARTS], block)
            out[:, cols] = value.astype(BF)
            tail = tail + dot_turned(high[j], block) + dot_turned(low[j], block)
        out[:, tail_at] = tail.astype(BF)
    last = pltpu.make_async_copy(out, layer_out, out_sem.at[0])
    last.start()

    def end(h, c):
        put(h).wait()
        return c

    lax.fori_loop(0, heads, end, 0)
    last.wait()


def maps(experts):
    rows = experts * CAP_DEV
    row = np.arange(rows)[:, None]
    place = np.arange(experts * ROWS)[None, :]
    same = row // CAP_DEV == place // ROWS
    slot, at = row % CAP_DEV, place % ROWS
    found = [
        same & (at == CAP_DEV + slot // PARTS) & (slot % PARTS == j) for j in range(PARTS)
    ] + [same & (at == slot)]
    found = np.stack(found).astype(np.float32)
    return jnp.asarray(found, BF), jnp.asarray(found.transpose(0, 2, 1), BF)


def on_device(
    tokens, state, norm_gain, w_recept, w_keys, w_values, decay_base, decay_first_matrix,
    decay_second_matrix, rate_base, rate_first_matrix, rate_second_matrix, head_gain, w_output,
    second_gain, route_ids, route_weights, expert_gate, expert_up, expert_down,
):
    devices = lax.axis_size("ep")
    group = devices // EXPERTS
    count, heads, width, _ = state.shape
    model = tokens.shape[1]
    inner = expert_gate.shape[1]
    mix = heads * width
    rows = EXPERTS * CAP_DEV
    packed_rows = EXPERTS * ROWS
    folded = PARTS * model // (PARTS + 1)
    mix_fold = PARTS * (mix // MIX_CHUNKS) // (PARTS + 1)
    out_fold = PARTS * (model // OUT_CHUNKS) // (PARTS + 1)
    unpack_m, pack_m = maps(EXPERTS // 2)
    vm = pl.BlockSpec(memory_space=pltpu.VMEM)
    hb = pl.BlockSpec(memory_space=pl.ANY)
    dma = pltpu.SemaphoreType.DMA
    weights = [
        w_recept, w_keys, w_values, decay_first_matrix, decay_second_matrix, rate_first_matrix,
        rate_second_matrix, w_output, expert_gate, expert_up, expert_down,
    ]
    smalls = [
        tokens, norm_gain[None], decay_base[None], rate_base[None], head_gain[None],
        second_gain[None], route_ids.T, route_weights.T, unpack_m, pack_m,
    ]
    st, ret, after, blend_w = pl.pallas_call(
        functools.partial(layer_kernel, devices),
        out_shape=(
            pltpu.VMEM((heads, count, width, width), F32),
            pltpu.VMEM((OUT_CHUNKS, EXPERTS, ROWS, out_fold), BF),
            pltpu.VMEM((count, model), F32),
            pltpu.VMEM((PARTS + 1, packed_rows, count), F32),
        ),
        in_specs=[hb] * 22,
        out_specs=(vm, vm, vm, vm),
        scratch_shapes=[
            *[pltpu.VMEM(w.shape, w.dtype) for w in smalls],
            *[pltpu.VMEM(w.shape, BF) for w in weights],
            pltpu.VMEM((count, model), BF),
            pltpu.VMEM((2, PARTS + 1, packed_rows, count), BF),
            pltpu.VMEM((4, count, mix), F32),
            pltpu.VMEM((heads, count, width), F32),
            pltpu.VMEM((heads, LANES, width), BF),
            pltpu.VMEM((mix, LANES), BF),
            pltpu.VMEM((mix, LANES), F32),
            pltpu.VMEM((mix // 2, LANES), F32),
            pltpu.VMEM((mix // 2, LANES), F32),
            pltpu.VMEM((count, mix), BF),
            pltpu.VMEM((2, EXPERTS, ROWS, folded), BF),
            pltpu.VMEM((EXPERTS, ROWS, folded), BF),
            pltpu.VMEM((MIX_CHUNKS, EXPERTS, ROWS, mix_fold), BF),
            pltpu.VMEM((MIX_CHUNKS, EXPERTS, ROWS, mix_fold), BF),
            pltpu.VMEM((rows, model), F32),
            pltpu.VMEM((group, rows, model), BF),
            pltpu.VMEM((group * rows // 2, inner), BF),
            pltpu.VMEM((OUT_CHUNKS, group, rows, model // OUT_CHUNKS), F32),
            pltpu.VMEM((OUT_CHUNKS, group, rows, model // OUT_CHUNKS), BF),
            pltpu.VMEM((OUT_CHUNKS, group, rows, model // OUT_CHUNKS), BF),
            pltpu.VMEM((OUT_CHUNKS, EXPERTS, ROWS, out_fold), BF),
            pltpu.VMEM((OUT_CHUNKS, EXPERTS, ROWS, out_fold), BF),
            dma((len(smalls),)),
            dma((8 + 3 * MIX_CHUNKS,)),
            dma((heads,)),
            dma,
            dma,
            dma,
            dma,
            dma((MIX_CHUNKS,)),
            dma((MIX_CHUNKS,)),
            dma((2, group)),
            dma((2, group)),
            dma((2, OUT_CHUNKS, group)),
            dma((2, OUT_CHUNKS, group)),
            dma((OUT_CHUNKS,)),
            dma((OUT_CHUNKS,)),
        ],
        compiler_params=pltpu.CompilerParams(
            collective_id=0, has_side_effects=True, vmem_limit_bytes=49 * 1024 * 1024
        ),
        name="layer",
    )(
        *smalls, state, w_recept, w_keys, w_values, decay_first_matrix, decay_second_matrix, rate_first_matrix, rate_second_matrix,
        w_output, expert_gate, expert_up, expert_down,
    )
    new_state, layer_out = pl.pallas_call(
        finish_kernel,
        out_shape=(
            jax.ShapeDtypeStruct(state.shape, F32),
            jax.ShapeDtypeStruct((count, model), BF),
        ),
        in_specs=[vm] * 4,
        out_specs=(hb, hb),
        scratch_shapes=[pltpu.VMEM((count, model), BF), dma((heads,)), dma((1,))],
        compiler_params=pltpu.CompilerParams(vmem_limit_bytes=4 * 1024 * 1024),
        name="finish",
    )(st, ret, after, blend_w)
    return (layer_out, new_state)


def solution(mesh):
    rep = P()
    in_specs = (
        P("ep", None), P("ep", None, None, None), *[rep] * 15,
        P(None, "ep"), P(None, "ep"), P("ep", None),
    )
    out_specs = (P("ep", None), P("ep", None, None, None))
    return jax.shard_map(
        on_device, mesh=mesh, in_specs=in_specs, out_specs=out_specs, check_vma=False
    )
```
